256 devices in a mesh: sp: 32 (over z, y), dp: 8 (over x, core).
Axes of the slice: x: 4, y: 4, z: 8, core: 2. Of those that a mesh axis runs over, the one named last changes fastest.
Arguments:
- cotangent: bfloat16 [8, 8192, 4096], P('dp', 'sp'), may hold values from -6 to 6
- up_pre: bfloat16 [8, 8192, 4096], P('dp', 'sp'), may hold values from -6 to 6
- value_pre: bfloat16 [8, 8192, 4096], P('dp', 'sp'), may hold values from -6 to 6
- spatial_weight: bfloat16 [32, 1024, 1024], P('sp', 'dp'), may hold values from -0.1875 to 0.1875
- spatial_bias: float32 [32, 1024], P('sp'), may hold values from 0.5 to 1.5
- value_gain: float32 [4096], replicated, may hold values from 0.1 to 1.9
Outputs:
- up_grad: bfloat16 [8, 8192, 4096], P('dp', 'sp')
- value_grad: bfloat16 [8, 8192, 4096], P('dp', 'sp')
- weight_grad: float32 [32, 1024, 1024], P('sp', 'dp')
- bias_grad: float32 [32, 1024], P('sp', 'dp')
- gain_grad: float32 [4096], replicated
The draws below stay inside these ranges and needn't reach their ends.
All inputs are finite; a program needn't handle non-finite values.
Results may differ from the reference program's by a relative error of at most 0.0064.
Values may be sent and summed in bfloat16 or wider, within the bound.
No kernel may reach another device: no remote copies, remote signals or barrier semaphores. Data moves between devices by JAX's collectives and lax.ppermute only.
A program may use at most 128 MiB of HBM per device.

```python
import math
import jax
import jax.numpy as jnp
from jax import lax

GROUPS = 32
GROUP = 128
BLOCK = 1024
WIDTH = 4096
SEQ = 8192
BATCH = 8


def shard_levels(key, shape, pieces, least, high):
    gain = 1.0
    for axis_at, parts in pieces:
        draws = jax.random.uniform(jax.random.fold_in(jax.random.fold_in(key, 6), axis_at), (parts,), jnp.float32, least / len(pieces), high / len(pieces))
        gain = gain * jnp.repeat(jnp.exp(draws), shape[axis_at] // parts).reshape((-1,) + (1,) * (len(shape) - 1 - axis_at))
    return gain


def centred(rng, dims, spread, most, pieces=(), dtype=jnp.bfloat16):
    values = jax.random.normal(rng, dims, jnp.float32) * spread
    if len(pieces) > 0:
        values = shard_levels(rng, dims, pieces, -0.22, 0.18) * values
    return jnp.clip(values, min=-most, max=most).astype(dtype)


def setup_inputs(seed: int = 0) -> dict:
    streams_of = jax.random.split(jax.random.key(seed), 7)
    return {
        "cotangent": centred(streams_of[0], (BATCH, SEQ, WIDTH), 1.0, 6.0, ((0, 8), (1, 32))),
        "up_pre": centred(streams_of[1], (BATCH, SEQ, WIDTH), 1.0, 6.0, ((0, 8), (1, 32))),
        "value_pre": centred(streams_of[2], (BATCH, SEQ, WIDTH), 1.0, 6.0, ((0, 8), (1, 32))),
        "spatial_weight": centred(streams_of[3], (GROUPS, BLOCK, BLOCK), BLOCK ** -0.5, 0.1875, ((0, 32), (1, 8))),
        "spatial_bias": jnp.clip(0.5 + 1.0 * jax.random.uniform(streams_of[4], (GROUPS, BLOCK), jnp.float32) ** shard_levels(streams_of[4], (GROUPS, BLOCK), ((0, 32),), -0.2, 0.2), 0.5, 1.5),
        "value_gain": jnp.clip(1.0 + 0.18 * jax.random.normal(streams_of[5], (WIDTH,), jnp.float32), 0.1, 1.9),
    }


norm_floor = 0.5
root_half = 1.0 / math.sqrt(2.0)
inv_root_tau = 1.0 / math.sqrt(2.0 * math.pi)

def gelu_slope(values):
    return 0.5 * (1.0 + jax.scipy.special.erf(values * root_half)) + values * jnp.exp(-0.5 * values * values) * inv_root_tau

def reference(cotangent, up_pre, value_pre, spatial_weight, spatial_bias, value_gain):
    weight_full = spatial_weight.astype(jnp.float32)
    bias_full = spatial_bias.astype(jnp.float32).T[None, :, :, None]
    gain_full = value_gain.astype(jnp.float32)
    block_shape = (SEQ // BLOCK, BLOCK, GROUPS, GROUP)

    def one_sequence(carried, inputs):
        grad_seq, up_seq, value_seq = inputs
        grad_tok = grad_seq.astype(jnp.float32)
        up_arg = up_seq.astype(jnp.float32)
        value_arg = value_seq.astype(jnp.float32)
        up_act = lax.optimization_barrier(jax.nn.gelu(up_arg, approximate=False).astype(jnp.bfloat16))
        value_act = jax.nn.gelu(value_arg, approximate=False)
        inv_rms = lax.rsqrt(lax.optimization_barrier(jnp.mean(value_act * value_act, axis=-1, keepdims=True)) + norm_floor)
        normed = value_act * inv_rms
        value_norm = lax.optimization_barrier((normed * gain_full).astype(jnp.bfloat16))
        gate_tok = lax.optimization_barrier((grad_tok * up_act.astype(jnp.float32)).astype(jnp.bfloat16))
        value_blocks = value_norm.astype(jnp.float32).reshape(block_shape)
        gate_blocks = gate_tok.astype(jnp.float32).reshape(block_shape)
        mixed_out = jnp.einsum('gpq,nqgc->npgc', weight_full, value_blocks) + bias_full
        mixed_out = lax.optimization_barrier(mixed_out.astype(jnp.bfloat16).reshape(SEQ, WIDTH))
        back_seq = jnp.einsum('gpq,npgc->nqgc', weight_full, gate_blocks)
        back_seq = lax.optimization_barrier(back_seq.astype(jnp.bfloat16).reshape(SEQ, WIDTH))
        weight_acc = carried[0] + jnp.einsum('npgc,nqgc->gpq', gate_blocks, value_blocks)
        bias_acc = carried[1] + lax.optimization_barrier(jnp.sum(gate_blocks, axis=(0, 3))).T
        up_mid = lax.optimization_barrier((grad_tok * mixed_out.astype(jnp.float32)).astype(jnp.bfloat16))
        up_out = (up_mid.astype(jnp.float32) * gelu_slope(up_arg)).astype(jnp.bfloat16)
        back_full = back_seq.astype(jnp.float32)
        gain_acc = carried[2] + lax.optimization_barrier(jnp.sum(back_full * normed, axis=0))
        scaled = back_full * gain_full
        value_slope = inv_rms * scaled - inv_rms ** 3 * value_act * lax.optimization_barrier(jnp.mean(scaled * value_act, axis=-1, keepdims=True))
        value_out = (value_slope * gelu_slope(value_arg)).astype(jnp.bfloat16)
        return ((weight_acc, bias_acc, gain_acc), (up_out, value_out))
    initial = (jnp.zeros((GROUPS, BLOCK, BLOCK), jnp.float32), jnp.zeros((GROUPS, BLOCK), jnp.float32), jnp.zeros((WIDTH,), jnp.float32))
    totals, outputs = lax.scan(one_sequence, initial, (cotangent, up_pre, value_pre))
    return (outputs[0], outputs[1], totals[0], totals[1], totals[2])
```

```python
import functools
import math

import jax
import jax.numpy as jnp
from jax import lax
from jax.experimental import pallas as pl
from jax.experimental.pallas import tpu as pltpu
from jax.sharding import Mesh
from jax.sharding import PartitionSpec as P

Z = "sp_0"
SP = ("sp_0", "sp_1")
DP = ("dp_0", "dp_1")
PLANE = ("dp_0", "dp_1", "sp_1")
Z_DP = ("sp_0", "dp_0", "dp_1")

norm_floor = 0.5
root_half = 1.0 / math.sqrt(2.0)
inv_root_tau = 1.0 / math.sqrt(2.0 * math.pi)
LANES = 128
F32 = jnp.float32
BF16 = jnp.bfloat16
VMEM_LIMIT = 56 * 1024 * 1024


def normal_cdf(x):
    return 0.5 * (1.0 + lax.erf(x * root_half))


def params(*semantics):
    return pltpu.CompilerParams(dimension_semantics=semantics, vmem_limit_bytes=VMEM_LIMIT)


def prologue_kernel(groups, cot_ref, up_ref, val_ref, gain_ref, out_ref, inv_ref, act_ref):
    rows = cot_ref.shape[0]

    def first(g, squares):
        at = pl.ds(pl.multiple_of(g * LANES, LANES), LANES)
        up = up_ref[:, at].astype(F32)
        up_act = (up * normal_cdf(up)).astype(BF16).astype(F32)
        out_ref[g, 0] = (cot_ref[:, at].astype(F32) * up_act).astype(BF16)
        val = val_ref[:, at].astype(F32)
        act = val * normal_cdf(val)
        act_ref[:, at] = act
        return squares + act * act

    squares = lax.fori_loop(0, groups, first, jnp.zeros((rows, LANES), F32), unroll=2)
    mean = jnp.sum(squares, axis=1, keepdims=True) * (1.0 / (groups * LANES))
    inv = lax.rsqrt(mean + norm_floor)
    inv_ref[...] = jnp.broadcast_to(inv, (rows, LANES))

    def second(g, carry):
        at = pl.ds(pl.multiple_of(g * LANES, LANES), LANES)
        out_ref[g, 1] = (act_ref[:, at] * inv * gain_ref[:, at]).astype(BF16)
        return carry

    lax.fori_loop(0, groups, second, 0, unroll=4)


def prologue(cot, up, val, gain, rows=32):
    toks, width = cot.shape
    groups = width // LANES
    row = pl.BlockSpec((rows, width), lambda i: (i, 0))
    return pl.pallas_call(
        functools.partial(prologue_kernel, groups),
        grid=(toks // rows,),
        in_specs=[row, row, row, pl.BlockSpec((1, width), lambda i: (0, 0))],
        out_specs=[
            pl.BlockSpec((groups, 2, rows, LANES), lambda i: (0, 0, i, 0)),
            pl.BlockSpec((rows, LANES), lambda i: (i, 0)),
        ],
        out_shape=[
            jax.ShapeDtypeStruct((groups, 2, toks, LANES), BF16),
            jax.ShapeDtypeStruct((toks, LANES), F32),
        ],
        scratch_shapes=[pltpu.VMEM((rows, width), F32)],
        compiler_params=params("arbitrary"),
        cost_estimate=pl.CostEstimate(
            flops=100 * toks * width, bytes_accessed=10 * toks * width, transcendentals=0
        ),
        name="prologue",
    )(cot, up, val, gain)


def slopes_kernel(up_ref, val_ref, up_slope_ref, val_slope_ref, act_ref):
    groups = up_ref.shape[1] // LANES

    def step(g, carry):
        at = pl.ds(pl.multiple_of(g * LANES, LANES), LANES)
        up = up_ref[:, at].astype(F32)
        up_slope_ref[:, at] = normal_cdf(up) + up * (jnp.exp(-0.5 * up * up) * inv_root_tau)
        val = val_ref[:, at].astype(F32)
        phi = normal_cdf(val)
        act_ref[:, at] = val * phi
        val_slope_ref[:, at] = phi + val * (jnp.exp(-0.5 * val * val) * inv_root_tau)
        return carry

    lax.fori_loop(0, groups, step, 0, unroll=2)


def slopes(up, val, rows=32):
    toks, width = up.shape
    row = pl.BlockSpec((rows, width), lambda i: (i, 0))
    out = jax.ShapeDtypeStruct((toks, width), F32)
    return pl.pallas_call(
        slopes_kernel,
        grid=(toks // rows,),
        in_specs=[row, row],
        out_specs=[row, row, row],
        out_shape=[out, out, out],
        compiler_params=params("arbitrary"),
        cost_estimate=pl.CostEstimate(
            flops=100 * toks * width, bytes_accessed=16 * toks * width, transcendentals=0
        ),
        name="slopes",
    )(up, val)


def gathered(ref, which, seqs, parts):
    return jnp.concatenate(
        [
            jnp.concatenate([ref[b * parts + y, which] for y in range(parts)], axis=0)
            for b in range(seqs)
        ],
        axis=1,
    )


def weight_grad_kernel(seqs, parts, slab, recv_ref, out_ref, value_ref):
    i = pl.program_id(0)

    @pl.when(i == 0)
    def _():
        for b in range(seqs):
            for y in range(parts):
                toks = recv_ref.shape[2]
                value_ref[y * toks : (y + 1) * toks, b * LANES : (b + 1) * LANES] = recv_ref[
                    b * parts + y, 1
                ]

    per = recv_ref.shape[2] // slab
    y = i // per
    at = pl.ds(pl.multiple_of((i % per) * slab, slab), slab)
    gate = jnp.concatenate([recv_ref[b * parts + y, 0, at] for b in range(seqs)], axis=1)
    across = (((1,), (1,)), ((), ()))
    out_ref[:slab] = lax.dot_general(
        gate, value_ref[...], across, preferred_element_type=F32
    ).astype(out_ref.dtype)
    sums = lax.dot_general(
        jnp.ones((8, gate.shape[1]), BF16), gate, across, preferred_element_type=F32
    )
    out_ref[slab:] = jnp.zeros((8, out_ref.shape[1]), out_ref.dtype)
    out_ref[slab:, :slab] = sums.astype(out_ref.dtype)


def weight_grads(recv, seqs, parts, slab, dtype):
    toks = recv.shape[2]
    block = parts * toks
    slabs = block // slab
    return pl.pallas_call(
        functools.partial(weight_grad_kernel, seqs, parts, slab),
        grid=(slabs,),
        in_specs=[pl.BlockSpec(recv.shape, lambda i: (0, 0, 0, 0))],
        out_specs=pl.BlockSpec((slab + 8, block), lambda i: (i, 0)),
        out_shape=jax.ShapeDtypeStruct((slabs * (slab + 8), block), dtype),
        scratch_shapes=[pltpu.VMEM((block, seqs * LANES), BF16)],
        compiler_params=params("arbitrary"),
        cost_estimate=pl.CostEstimate(
            flops=2 * block * block * seqs * LANES, bytes_accessed=8 * block * block, transcendentals=0
        ),
        name="weight_grads",
    )(recv)


def mix_kernel(seqs, parts, recv_ref, w_ref, bias_ref, out_ref, gain_ref, gate_ref, value_ref):
    y = pl.program_id(0)
    toks = recv_ref.shape[2]

    @pl.when(y == 0)
    def _():
        gain_ref[...] = jnp.zeros_like(gain_ref)
        for b in range(seqs):
            for k in range(parts):
                rows, cols = pl.ds(k * toks, toks), pl.ds(b * LANES, LANES)
                gate_ref[rows, cols] = recv_ref[b * parts + k, 0]
                value_ref[rows, cols] = recv_ref[b * parts + k, 1]

    at = pl.ds(pl.multiple_of(y * toks, toks), toks)
    back = lax.dot_general(
        w_ref[:, at], gate_ref[...], (((0,), (0,)), ((), ())), preferred_element_type=F32
    ).astype(BF16)
    terms = back.astype(F32) * value_ref[at].astype(F32)
    total = jnp.zeros((8, LANES), F32)
    for b in range(seqs):
        out_ref[b, 0, 1] = back[:, b * LANES : (b + 1) * LANES]
        total += jnp.sum(
            terms[:, b * LANES : (b + 1) * LANES].reshape(toks // 8, 8, LANES), axis=0
        )
    gain_ref[...] += total
    mixed = jnp.dot(w_ref[at], value_ref[...], preferred_element_type=F32)
    mixed = (mixed + bias_ref[at, :1]).astype(BF16)
    for b in range(seqs):
        out_ref[b, 0, 0] = mixed[:, b * LANES : (b + 1) * LANES]


def mix(recv, w, bias, seqs, parts):
    toks = recv.shape[2]
    block = parts * toks
    out, gain = pl.pallas_call(
        functools.partial(mix_kernel, seqs, parts),
        grid=(parts,),
        in_specs=[
            pl.BlockSpec(recv.shape, lambda y: (0, 0, 0, 0)),
            pl.BlockSpec(w.shape, lambda y: (0, 0)),
            pl.BlockSpec(bias.shape, lambda y: (0, 0)),
        ],
        out_specs=[
            pl.BlockSpec((seqs, 1, 2, toks, LANES), lambda y: (0, y, 0, 0, 0)),
            pl.BlockSpec((8, LANES), lambda y: (0, 0)),
        ],
        out_shape=[
            jax.ShapeDtypeStruct((seqs, parts, 2, toks, LANES), BF16),
            jax.ShapeDtypeStruct((8, LANES), F32),
        ],
        scratch_shapes=[pltpu.VMEM((block, seqs * LANES), BF16)] * 2,
        compiler_params=params("arbitrary"),
        cost_estimate=pl.CostEstimate(
            flops=4 * block * block * seqs * LANES, bytes_accessed=10 * block * block, transcendentals=0
        ),
        name="mix",
    )(recv, w, bias)
    return out.reshape(recv.shape), gain


def epilogue_kernel(
    groups, recv_ref, cot_ref, up_slope_ref, val_slope_ref, act_ref, inv_ref, gain_ref, up_ref, val_ref
):
    rows = cot_ref.shape[0]

    def first(g, dots):
        at = pl.ds(pl.multiple_of(g * LANES, LANES), LANES)
        mid = (cot_ref[:, at].astype(F32) * recv_ref[g, 0].astype(F32)).astype(BF16)
        up_ref[:, at] = (mid.astype(F32) * up_slope_ref[:, at]).astype(BF16)
        scaled = recv_ref[g, 1].astype(F32) * gain_ref[:, at]
        return dots + scaled * act_ref[:, at]

    dots = lax.fori_loop(0, groups, first, jnp.zeros((rows, LANES), F32), unroll=2)
    mean = jnp.sum(dots, axis=1, keepdims=True) * (1.0 / (groups * LANES))
    inv = inv_ref[...]
    pull = inv * inv * inv * mean

    def second(g, carry):
        at = pl.ds(pl.multiple_of(g * LANES, LANES), LANES)
        scaled = recv_ref[g, 1].astype(F32) * gain_ref[:, at]
        slope = inv * scaled - pull * act_ref[:, at]
        val_ref[:, at] = (slope * val_slope_ref[:, at]).astype(BF16)
        return carry

    lax.fori_loop(0, groups, second, 0, unroll=4)


def epilogue(recv, cot, up_slope, val_slope, act, inv, gain, rows=32):
    toks, width = cot.shape
    groups = width // LANES
    row = pl.BlockSpec((rows, width), lambda i: (i, 0))
    out = jax.ShapeDtypeStruct((toks, width), BF16)
    return pl.pallas_call(
        functools.partial(epilogue_kernel, groups),
        grid=(toks // rows,),
        in_specs=[
            pl.BlockSpec((groups, 2, rows, LANES), lambda i: (0, 0, i, 0)),
            row,
            row,
            row,
            row,
            pl.BlockSpec((rows, LANES), lambda i: (i, 0)),
            pl.BlockSpec((1, width), lambda i: (0, 0)),
        ],
        out_specs=[row, row],
        out_shape=[out, out],
        compiler_params=params("arbitrary"),
        cost_estimate=pl.CostEstimate(
            flops=20 * toks * width, bytes_accessed=22 * toks * width, transcendentals=0
        ),
        name="epilogue",
    )(recv, cot, up_slope, val_slope, act, inv, gain)


def shards(cotangent, up_pre, value_pre, spatial_weight, spatial_bias, value_gain):
    planes = lax.axis_size(Z)
    seqs = lax.axis_size(DP)
    parts = lax.axis_size("sp_1")
    slab = spatial_weight.shape[1]
    cot, up, val = cotangent[0], up_pre[0], value_pre[0]
    gain = value_gain[None]

    swap = [(k * seqs + a, a * seqs + k) for k in range(planes) for a in range(seqs)]
    high = spatial_bias.astype(BF16)
    middle = (spatial_bias - high.astype(F32)).astype(BF16)
    low = (spatial_bias - high.astype(F32) - middle.astype(F32)).astype(BF16)
    pad = jnp.zeros((5, slab * seqs), BF16)
    own = jnp.concatenate([spatial_weight[0], high, middle, low, pad], axis=0)
    own = lax.ppermute(own, Z_DP, swap)
    bias = jnp.sum(own[slab : slab + 3].astype(F32), axis=0)
    weights = lax.all_gather(own[:slab], Z, axis=0, tiled=True)

    sent, inv = prologue(cot, up, val, gain)
    recv = lax.all_to_all(sent, PLANE, split_axis=0, concat_axis=0, tiled=True)
    up_slope, val_slope, act = slopes(up, val)

    grads = weight_grads(recv, seqs, parts, slab, F32)
    grads = lax.psum_scatter(grads, Z, scatter_dimension=0, tiled=True)
    grads = lax.ppermute(grads, Z_DP, swap)

    bias_col = jnp.broadcast_to(bias[:, None], (bias.shape[0], LANES))
    back, gain_part = mix(recv, weights, bias_col, seqs, parts)
    back = lax.all_to_all(back, PLANE, split_axis=0, concat_axis=0, tiled=True)
    gain_part = lax.psum(jnp.sum(gain_part, axis=0, keepdims=True), Z)
    gain_grad = lax.all_gather(gain_part, PLANE, axis=0, tiled=True).reshape(-1) / value_gain
    up_grad, value_grad = epilogue(back, cot, up_slope, val_slope, act, inv, gain)
    return (
        up_grad[None],
        value_grad[None],
        grads[None, :slab].astype(F32),
        grads[slab : slab + 1, :slab].astype(F32),
        gain_grad,
    )


def solution(mesh):
    torus = Mesh(mesh.devices.reshape(8, 4, 4, 2), ("sp_0", "sp_1", "dp_0", "dp_1"))
    in_specs = (
        P(DP, SP, None),
        P(DP, SP, None),
        P(DP, SP, None),
        P(SP, DP, None),
        P(SP, None),
        P(),
    )
    out_specs = (P(DP, SP, None), P(DP, SP, None), P(SP, DP, None), P(SP, DP), P())
    return jax.shard_map(
        shards, mesh=torus, in_specs=in_specs, out_specs=out_specs, check_vma=False
    )
```

```python
import functools
import math

import jax
import jax.numpy as jnp
from jax import lax
from jax.experimental import pallas as pl
from jax.experimental.pallas import tpu as pltpu
from jax.sharding import Mesh
from jax.sharding import PartitionSpec as P

Z = "sp_0"
SP = ("sp_0", "sp_1")
DP = ("dp_0", "dp_1")
PLANE = ("dp_0", "dp_1", "sp_1")
Z_DP = ("sp_0", "dp_0", "dp_1")

norm_floor = 0.5
root_half = 1.0 / math.sqrt(2.0)
inv_root_tau = 1.0 / math.sqrt(2.0 * math.pi)
LANES = 128
F32 = jnp.float32
BF16 = jnp.bfloat16


def normal_cdf(x):
    return 0.5 * (1.0 + lax.erf(x * root_half))


def params(mib):
    return pltpu.CompilerParams(
        dimension_semantics=("arbitrary",), vmem_limit_bytes=mib * 1024 * 1024
    )


def prologue_kernel(groups, cot_ref, up_ref, val_ref, gain_ref, out_ref, inv_ref, act_ref):
    rows = cot_ref.shape[0]

    def first(g, squares):
        at = pl.ds(pl.multiple_of(g * LANES, LANES), LANES)
        up = up_ref[:, at].astype(F32)
        up_act = (up * normal_cdf(up)).astype(BF16).astype(F32)
        out_ref[g, 0] = (cot_ref[:, at].astype(F32) * up_act).astype(BF16)
        val = val_ref[:, at].astype(F32)
        act = val * normal_cdf(val)
        act_ref[:, at] = act
        return squares + act * act

    squares = lax.fori_loop(0, groups, first, jnp.zeros((rows, LANES), F32), unroll=2)
    mean = jnp.sum(squares, axis=1, keepdims=True) * (1.0 / (groups * LANES))
    inv = lax.rsqrt(mean + norm_floor)
    inv_ref[...] = jnp.broadcast_to(inv, (rows, LANES))

    def second(g, carry):
        at = pl.ds(pl.multiple_of(g * LANES, LANES), LANES)
        out_ref[g, 1] = (act_ref[:, at] * inv * gain_ref[:, at]).astype(BF16)
        return carry

    lax.fori_loop(0, groups, second, 0, unroll=4)


def prologue(cot, up, val, gain, rows=32):
    toks, width = cot.shape
    groups = width // LANES
    row = pl.BlockSpec((rows, width), lambda i: (i, 0))
    return pl.pallas_call(
        functools.partial(prologue_kernel, groups),
        grid=(toks // rows,),
        in_specs=[row, row, row, pl.BlockSpec((1, width), lambda i: (0, 0))],
        out_specs=[
            pl.BlockSpec((groups, 2, rows, LANES), lambda i: (0, 0, i, 0)),
            pl.BlockSpec((rows, LANES), lambda i: (i, 0)),
        ],
        out_shape=[
            jax.ShapeDtypeStruct((groups, 2, toks, LANES), BF16),
            jax.ShapeDtypeStruct((toks, LANES), F32),
        ],
        scratch_shapes=[pltpu.VMEM((rows, width), F32)],
        compiler_params=params(60),
        cost_estimate=pl.CostEstimate(
            flops=100 * toks * width, bytes_accessed=10 * toks * width, transcendentals=0
        ),
        name="prologue",
    )(cot, up, val, gain)


def slopes_kernel(up_ref, val_ref, up_slope_ref, val_slope_ref, act_ref):
    groups = up_ref.shape[1] // LANES

    def step(g, carry):
        at = pl.ds(pl.multiple_of(g * LANES, LANES), LANES)
        up = up_ref[:, at].astype(F32)
        up_slope_ref[:, at] = normal_cdf(up) + up * (jnp.exp(-0.5 * up * up) * inv_root_tau)
        val = val_ref[:, at].astype(F32)
        phi = normal_cdf(val)
        act_ref[:, at] = val * phi
        val_slope_ref[:, at] = phi + val * (jnp.exp(-0.5 * val * val) * inv_root_tau)
        return carry

    lax.fori_loop(0, groups, step, 0, unroll=2)


def slopes(up, val, rows=32):
    toks, width = up.shape
    row = pl.BlockSpec((rows, width), lambda i: (i, 0))
    out = jax.ShapeDtypeStruct((toks, width), F32)
    return pl.pallas_call(
        slopes_kernel,
        grid=(toks // rows,),
        in_specs=[row, row],
        out_specs=[row, row, row],
        out_shape=[out, out, out],
        compiler_params=params(60),
        cost_estimate=pl.CostEstimate(
            flops=100 * toks * width, bytes_accessed=16 * toks * width, transcendentals=0
        ),
        name="slopes",
    )(up, val)


def core_kernel(
    seqs, parts, recv_ref, w_ref, bias_ref, grad_ref, out_ref, sums_ref, gate_ref, value_ref
):
    y = pl.program_id(0)
    toks = recv_ref.shape[2]

    @pl.when(y == 0)
    def _():
        for b in range(seqs):
            for k in range(parts):
                rows, cols = pl.ds(k * toks, toks), pl.ds(b * LANES, LANES)
                gate_ref[rows, cols] = recv_ref[b * parts + k, 0]
                value_ref[rows, cols] = recv_ref[b * parts + k, 1]

    at = pl.ds(pl.multiple_of(y * toks, toks), toks)
    across = (((1,), (1,)), ((), ()))
    gate = gate_ref[at]
    grad_ref[...] = lax.dot_general(
        gate, value_ref[...], across, preferred_element_type=F32
    ).astype(grad_ref.dtype)
    ones = jnp.ones((8, gate.shape[1]), BF16)
    shift = pl.ds(pl.multiple_of(LANES + y * toks, LANES), toks)
    sums_ref[:, shift] = lax.dot_general(ones, gate, across, preferred_element_type=F32)
    back = lax.dot_general(
        w_ref[:, at], gate_ref[...], (((0,), (0,)), ((), ())), preferred_element_type=F32
    ).astype(BF16)
    terms = back.astype(F32) * value_ref[at].astype(F32)
    total = jnp.zeros((8, LANES), F32)
    for b in range(seqs):
        out_ref[b, 0, 1] = back[:, b * LANES : (b + 1) * LANES]
        total += jnp.sum(
            terms[:, b * LANES : (b + 1) * LANES].reshape(toks // 8, 8, LANES), axis=0
        )
    total = jnp.broadcast_to(jnp.sum(total, axis=0, keepdims=True), (8, LANES))

    @pl.when(y == 0)
    def _():
        sums_ref[:, :LANES] = total

    @pl.when(y > 0)
    def _():
        sums_ref[:, :LANES] += total

    mixed = jnp.dot(w_ref[at], value_ref[...], preferred_element_type=F32)
    mixed = (mixed + bias_ref[at, :1]).astype(BF16)
    for b in range(seqs):
        out_ref[b, 0, 0] = mixed[:, b * LANES : (b + 1) * LANES]


def core(recv, w, bias, seqs, parts):
    toks = recv.shape[2]
    block = parts * toks
    grads, out, sums = pl.pallas_call(
        functools.partial(core_kernel, seqs, parts),
        grid=(parts,),
        in_specs=[
            pl.BlockSpec(recv.shape, lambda y: (0, 0, 0, 0)),
            pl.BlockSpec(w.shape, lambda y: (0, 0)),
            pl.BlockSpec(bias.shape, lambda y: (0, 0)),
        ],
        out_specs=[
            pl.BlockSpec((toks, block), lambda y: (y, 0)),
            pl.BlockSpec((seqs, 1, 2, toks, LANES), lambda y: (0, y, 0, 0, 0)),
            pl.BlockSpec((8, LANES + block), lambda y: (0, 0)),
        ],
        out_shape=[
            jax.ShapeDtypeStruct((block, block), BF16),
            jax.ShapeDtypeStruct((seqs, parts, 2, toks, LANES), BF16),
            jax.ShapeDtypeStruct((8, LANES + block), F32),
        ],
        scratch_shapes=[pltpu.VMEM((block, seqs * LANES), BF16)] * 2,
        compiler_params=params(60),
        cost_estimate=pl.CostEstimate(
            flops=6 * block * block * seqs * LANES, bytes_accessed=12 * block * block, transcendentals=0
        ),
        name="core",
    )(recv, w, bias)
    return grads, out.reshape(recv.shape), sums[:1]


def epilogue_kernel(
    groups, recv_ref, cot_ref, up_slope_ref, val_slope_ref, act_ref, inv_ref, gain_ref, up_ref, val_ref
):
    rows = cot_ref.shape[0]

    def first(g, dots):
        at = pl.ds(pl.multiple_of(g * LANES, LANES), LANES)
        mid = (cot_ref[:, at].astype(F32) * recv_ref[g, 0].astype(F32)).astype(BF16)
        up_ref[:, at] = (mid.astype(F32) * up_slope_ref[:, at]).astype(BF16)
        scaled = recv_ref[g, 1].astype(F32) * gain_ref[:, at]
        return dots + scaled * act_ref[:, at]

    dots = lax.fori_loop(0, groups, first, jnp.zeros((rows, LANES), F32), unroll=2)
    mean = jnp.sum(dots, axis=1, keepdims=True) * (1.0 / (groups * LANES))
    inv = inv_ref[...]
    pull = inv * inv * inv * mean

    def second(g, carry):
        at = pl.ds(pl.multiple_of(g * LANES, LANES), LANES)
        scaled = recv_ref[g, 1].astype(F32) * gain_ref[:, at]
        slope = inv * scaled - pull * act_ref[:, at]
        val_ref[:, at] = (slope * val_slope_ref[:, at]).astype(BF16)
        return carry

    lax.fori_loop(0, groups, second, 0, unroll=4)


def epilogue(recv, cot, up_slope, val_slope, act, inv, gain, rows=32):
    toks, width = cot.shape
    groups = width // LANES
    row = pl.BlockSpec((rows, width), lambda i: (i, 0))
    out = jax.ShapeDtypeStruct((toks, width), BF16)
    return pl.pallas_call(
        functools.partial(epilogue_kernel, groups),
        grid=(toks // rows,),
        in_specs=[
            pl.BlockSpec((groups, 2, rows, LANES), lambda i: (0, 0, i, 0)),
            row,
            row,
            row,
            row,
            pl.BlockSpec((rows, LANES), lambda i: (i, 0)),
            pl.BlockSpec((1, width), lambda i: (0, 0)),
        ],
        out_specs=[row, row],
        out_shape=[out, out],
        compiler_params=params(60),
        cost_estimate=pl.CostEstimate(
            flops=20 * toks * width, bytes_accessed=22 * toks * width, transcendentals=0
        ),
        name="epilogue",
    )(recv, cot, up_slope, val_slope, act, inv, gain)


def pack_kernel(seqs, parts, sums_ref, out_ref):
    out_ref[...] = jnp.zeros_like(out_ref)
    for a in range(seqs):
        at = slice((a + 1) * LANES, (a + 2) * LANES)
        for y in range(parts):
            out_ref[a * parts + y, :1] = sums_ref[:, :LANES]
            out_ref[a * parts + y, 1:2] = sums_ref[:, at]


def pack(sums, seqs, parts):
    shape = (seqs * parts, 8, LANES)
    return pl.pallas_call(
        functools.partial(pack_kernel, seqs, parts),
        grid=(1,),
        in_specs=[pl.BlockSpec(sums.shape, lambda i: (0, 0))],
        out_specs=pl.BlockSpec(shape, lambda i: (0, 0, 0)),
        out_shape=jax.ShapeDtypeStruct(shape, F32),
        compiler_params=params(60),
        name="pack",
    )(sums)


def shards(cotangent, up_pre, value_pre, spatial_weight, spatial_bias, value_gain):
    planes = lax.axis_size(Z)
    seqs = lax.axis_size(DP)
    parts = lax.axis_size("sp_1")
    block = spatial_weight.shape[2]
    cot, up, val = cotangent[0], up_pre[0], value_pre[0]
    gain = value_gain[None]
    swap = [(k * seqs + a, a * seqs + k) for k in range(planes) for a in range(seqs)]

    def exchange(x):
        return lax.all_to_all(x, PLANE, split_axis=0, concat_axis=0, tiled=True)

    weights = lax.ppermute(spatial_weight[0], Z_DP, swap)
    weights = lax.all_gather(weights, Z, axis=0, tiled=True)
    sent, inv = prologue(cot, up, val, gain)
    recv = exchange(sent)
    bias = lax.ppermute(spatial_bias, Z_DP, swap)
    bias = jnp.broadcast_to(bias.reshape(block, 1), (block, LANES))
    up_slope, val_slope, act = slopes(up, val)
    grads, back, sums = core(recv, weights, bias, seqs, parts)
    grads = lax.psum_scatter(grads, Z, scatter_dimension=0, tiled=True)
    back = exchange(back)
    sums = lax.psum(sums, Z)
    grads = lax.ppermute(grads, Z_DP, swap)
    small = pack(sums, seqs, parts)
    small = exchange(small)
    gain_grad = small[:, 0].reshape(-1) / value_gain
    mine = lax.axis_index(Z) * parts + lax.axis_index("sp_1")
    bias_grad = lax.dynamic_slice_in_dim(small, mine, 1, axis=0)[:, 1]
    up_grad, value_grad = epilogue(back, cot, up_slope, val_slope, act, inv, gain)
    return (up_grad[None], value_grad[None], grads[None].astype(F32), bias_grad, gain_grad)


def solution(mesh):
    torus = Mesh(mesh.devices.reshape(8, 4, 4, 2), ("sp_0", "sp_1", "dp_0", "dp_1"))
    in_specs = (
        P(DP, SP, None),
        P(DP, SP, None),
        P(DP, SP, None),
        P(SP, DP, None),
        P(SP, None),
        P(),
    )
    out_specs = (P(DP, SP, None), P(DP, SP, None), P(SP, DP, None), P(SP, DP), P())
    return jax.shard_map(
        shards, mesh=torus, in_specs=in_specs, out_specs=out_specs, check_vma=False
    )
```

```python
import functools
import math

import jax
import jax.numpy as jnp
from jax import lax
from jax.experimental import pallas as pl
from jax.experimental.pallas import tpu as pltpu
from jax.sharding import Mesh
from jax.sharding import PartitionSpec as P

Z = "sp_0"
SP = ("sp_0", "sp_1")
DP = ("dp_0", "dp_1")
PLANE = ("dp_0", "dp_1", "sp_1")
Z_DP = ("sp_0", "dp_0", "dp_1")

norm_floor = 0.5
root_half = 1.0 / math.sqrt(2.0)
inv_root_tau = 1.0 / math.sqrt(2.0 * math.pi)
LANES = 128
F32 = jnp.float32
BF16 = jnp.bfloat16


def normal_cdf(x):
    return 0.5 * (1.0 + lax.erf(x * root_half))


def params(mib):
    return pltpu.CompilerParams(
        dimension_semantics=("arbitrary",), vmem_limit_bytes=mib * 1024 * 1024
    )


def prologue_kernel(groups, cot_ref, up_ref, val_ref, gain_ref, out_ref, inv_ref, act_ref):
    rows = cot_ref.shape[0]

    def first(g, squares):
        at = pl.ds(pl.multiple_of(g * LANES, LANES), LANES)
        up = up_ref[:, at].astype(F32)
        up_act = (up * normal_cdf(up)).astype(BF16).astype(F32)
        out_ref[g, 0] = (cot_ref[:, at].astype(F32) * up_act).astype(BF16)
        val = val_ref[:, at].astype(F32)
        act = val * normal_cdf(val)
        act_ref[:, at] = act
        return squares + act * act

    squares = lax.fori_loop(0, groups, first, jnp.zeros((rows, LANES), F32), unroll=2)
    mean = jnp.sum(squares, axis=1, keepdims=True) * (1.0 / (groups * LANES))
    inv = lax.rsqrt(mean + norm_floor)
    inv_ref[...] = jnp.broadcast_to(inv, (rows, LANES))

    def second(g, carry):
        at = pl.ds(pl.multiple_of(g * LANES, LANES), LANES)
        out_ref[g, 1] = (act_ref[:, at] * inv * gain_ref[:, at]).astype(BF16)
        return carry

    lax.fori_loop(0, groups, second, 0, unroll=4)


def prologue(cot, up, val, gain, rows=32):
    toks, width = cot.shape
    groups = width // LANES
    row = pl.BlockSpec((rows, width), lambda i: (i, 0))
    return pl.pallas_call(
        functools.partial(prologue_kernel, groups),
        grid=(toks // rows,),
        in_specs=[row, row, row, pl.BlockSpec((1, width), lambda i: (0, 0))],
        out_specs=[
            pl.BlockSpec((groups, 2, rows, LANES), lambda i: (0, 0, i, 0)),
            pl.BlockSpec((rows, LANES), lambda i: (i, 0)),
        ],
        out_shape=[
            jax.ShapeDtypeStruct((groups, 2, toks, LANES), BF16),
            jax.ShapeDtypeStruct((toks, LANES), F32),
        ],
        scratch_shapes=[pltpu.VMEM((rows, width), F32)],
        compiler_params=params(60),
        cost_estimate=pl.CostEstimate(
            flops=100 * toks * width, bytes_accessed=10 * toks * width, transcendentals=0
        ),
        name="prologue",
    )(cot, up, val, gain)


def slopes_kernel(up_ref, val_ref, up_slope_ref, val_slope_ref, act_ref):
    groups = up_ref.shape[1] // LANES

    def step(g, carry):
        at = pl.ds(pl.multiple_of(g * LANES, LANES), LANES)
        up = up_ref[:, at].astype(F32)
        up_slope = normal_cdf(up) + up * (jnp.exp(-0.5 * up * up) * inv_root_tau)
        up_slope_ref[:, at] = up_slope.astype(BF16)
        val = val_ref[:, at].astype(F32)
        phi = normal_cdf(val)
        act_ref[:, at] = (val * phi).astype(BF16)
        val_slope = phi + val * (jnp.exp(-0.5 * val * val) * inv_root_tau)
        val_slope_ref[:, at] = val_slope.astype(BF16)
        return carry

    lax.fori_loop(0, groups, step, 0, unroll=2)


def slopes(up, val, rows=32):
    toks, width = up.shape
    row = pl.BlockSpec((rows, width), lambda i: (i, 0))
    out = jax.ShapeDtypeStruct((toks, width), BF16)
    return pl.pallas_call(
        slopes_kernel,
        grid=(toks // rows,),
        in_specs=[row, row],
        out_specs=[row, row, row],
        out_shape=[out, out, out],
        compiler_params=params(60),
        cost_estimate=pl.CostEstimate(
            flops=100 * toks * width, bytes_accessed=16 * toks * width, transcendentals=0
        ),
        name="slopes",
    )(up, val)


def mix_kernel(seqs, parts, *refs):
    recv_ref, *w_refs = refs[: 1 + seqs]
    bias_ref, out_ref, sums_ref, gate_ref, value_ref, w_ref, mixed_ref, back_ref, sems = refs[1 + seqs :]
    toks = recv_ref.shape[2]
    block = parts * toks
    slab = block // seqs
    key = order_key()
    gate_sem, value_sem, w_sem, back_sem, mixed_sem = (sems.at[k] for k in range(5))
    for b in range(seqs):
        cols = slice(b * LANES, (b + 1) * LANES)
        pieces = slice(b * parts, (b + 1) * parts)
        pltpu.make_async_copy(recv_ref.at[pieces, 0], gate_ref.at[:, :, cols], gate_sem).start()
    for d in range(seqs):
        rows = pl.ds(pl.multiple_of((d ^ key) * slab, slab), slab)
        pltpu.make_async_copy(w_refs[d], w_ref.at[rows], w_sem).start()
    for b in range(seqs):
        cols = slice(b * LANES, (b + 1) * LANES)
        pieces = slice(b * parts, (b + 1) * parts)
        pltpu.make_async_copy(recv_ref.at[pieces, 1], value_ref.at[:, :, cols], value_sem).start()
    pltpu.make_async_copy(gate_ref, gate_ref, gate_sem).wait()
    pltpu.make_async_copy(w_ref, w_ref, w_sem).wait()

    gate = gate_ref[...].reshape(block, seqs * LANES)
    across = (((1,), (1,)), ((), ()))
    ones = jnp.ones((8, seqs * LANES), BF16)
    bias_sums = lax.dot_general(ones, gate, across, preferred_element_type=F32)
    sums_ref[:, LANES:] = bias_sums[:1]

    def back_step(y, carry):
        at = pl.ds(pl.multiple_of(y * toks, toks), toks)
        back_ref[y] = lax.dot_general(
            w_ref[:, at],
            gate_ref[...].reshape(block, seqs * LANES),
            (((0,), (0,)), ((), ())),
            preferred_element_type=F32,
        ).astype(BF16)
        for b in range(seqs):
            cols = slice(b * LANES, (b + 1) * LANES)
            pltpu.make_async_copy(back_ref.at[y, :, cols], out_ref.at[b, y, 1], back_sem).start()
        return carry

    lax.fori_loop(0, parts, back_step, 0)
    pltpu.make_async_copy(value_ref, value_ref, value_sem).wait()

    def mixed_step(y, total):
        at = pl.ds(pl.multiple_of(y * toks, toks), toks)
        mixed = jnp.dot(
            w_ref[at], value_ref[...].reshape(block, seqs * LANES), preferred_element_type=F32
        )
        mixed_ref[y] = (mixed + bias_ref[at, :1]).astype(BF16)
        for b in range(seqs):
            cols = slice(b * LANES, (b + 1) * LANES)
            pltpu.make_async_copy(mixed_ref.at[y, :, cols], out_ref.at[b, y, 0], mixed_sem).start()
            terms = back_ref[y, :, cols].astype(F32) * value_ref[y, :, cols].astype(F32)
            total += jnp.sum(terms.reshape(toks // 8, 8, LANES), axis=0)
        return total

    total = lax.fori_loop(0, parts, mixed_step, jnp.zeros((8, LANES), F32))
    sums_ref[:, :LANES] = jnp.sum(total, axis=0, keepdims=True)
    pltpu.make_async_copy(back_ref, back_ref, back_sem).wait()
    pltpu.make_async_copy(mixed_ref, mixed_ref, mixed_sem).wait()


def order_key():
    return lax.axis_index(Z) ^ (lax.axis_index("dp_0") * 2 + lax.axis_index("dp_1"))


ANY = pl.BlockSpec(memory_space=pl.ANY)
VMEM = pl.BlockSpec(memory_space=pltpu.VMEM)


def mix(recv, pieces, bias, seqs, parts):
    toks = recv.shape[2]
    block = parts * toks
    flat = pltpu.VMEM((parts, toks, seqs * LANES), BF16)
    out, sums = pl.pallas_call(
        functools.partial(mix_kernel, seqs, parts),
        in_specs=[ANY] * (1 + seqs) + [VMEM],
        out_specs=[ANY, VMEM],
        out_shape=[
            jax.ShapeDtypeStruct((seqs, parts, 2, toks, LANES), BF16),
            jax.ShapeDtypeStruct((1, LANES + block), F32),
        ],
        scratch_shapes=[
            flat,
            flat,
            pltpu.VMEM((block, block), BF16),
            flat,
            flat,
            pltpu.SemaphoreType.DMA((5,)),
        ],
        compiler_params=pltpu.CompilerParams(vmem_limit_bytes=60 * 1024 * 1024),
        cost_estimate=pl.CostEstimate(
            flops=4 * block * block * seqs * LANES, bytes_accessed=10 * block * block, transcendentals=0
        ),
        name="mix",
    )(recv, *pieces, bias)
    return out.reshape(recv.shape), sums


def grads_kernel(seqs, parts, recv_ref, *refs):
    outs = refs[:seqs]
    gate_ref, value_ref, grad_ref, sems = refs[seqs:]
    toks = recv_ref.shape[2]
    block = parts * toks
    slab = block // seqs
    key = order_key()
    for b in range(seqs):
        cols = slice(b * LANES, (b + 1) * LANES)
        pieces = slice(b * parts, (b + 1) * parts)
        pltpu.make_async_copy(recv_ref.at[pieces, 0], gate_ref.at[:, :, cols], sems.at[0]).start()
        pltpu.make_async_copy(recv_ref.at[pieces, 1], value_ref.at[:, :, cols], sems.at[1]).start()
    pltpu.make_async_copy(gate_ref, gate_ref, sems.at[0]).wait()
    pltpu.make_async_copy(value_ref, value_ref, sems.at[1]).wait()

    def step(y, carry):
        grad = lax.dot_general(
            gate_ref[...].reshape(block, seqs * LANES),
            value_ref[y],
            (((1,), (1,)), ((), ())),
            preferred_element_type=F32,
        )
        grad_ref[y] = grad.astype(BF16)
        at = pl.ds(pl.multiple_of(y * toks, toks), toks)
        for d in range(seqs):
            rows = pl.ds(pl.multiple_of((d ^ key) * slab, slab), slab)
            pltpu.make_async_copy(grad_ref.at[y, rows], outs[d].at[:, at], sems.at[2]).start()
        return carry

    lax.fori_loop(0, parts, step, 0)
    pltpu.make_async_copy(grad_ref, grad_ref, sems.at[2]).wait()


def weight_grads(recv, seqs, parts):
    toks = recv.shape[2]
    block = parts * toks
    flat = pltpu.VMEM((parts, toks, seqs * LANES), BF16)
    return pl.pallas_call(
        functools.partial(grads_kernel, seqs, parts),
        in_specs=[ANY],
        out_specs=[ANY] * seqs,
        out_shape=[jax.ShapeDtypeStruct((block // seqs, block), BF16)] * seqs,
        scratch_shapes=[
            flat,
            flat,
            pltpu.VMEM((parts, block, toks), BF16),
            pltpu.SemaphoreType.DMA((3,)),
        ],
        compiler_params=pltpu.CompilerParams(vmem_limit_bytes=60 * 1024 * 1024),
        cost_estimate=pl.CostEstimate(
            flops=2 * block * block * seqs * LANES, bytes_accessed=6 * block * block, transcendentals=0
        ),
        name="weight_grads",
    )(recv)


def add_kernel(*refs):
    *ins, out_ref = refs
    out_ref[...] = sum(r[...].astype(F32) for r in ins).astype(BF16)


def add(pieces, rows=32):
    height, width = pieces[0].shape
    row = pl.BlockSpec((rows, width), lambda i: (i, 0))
    return pl.pallas_call(
        add_kernel,
        grid=(height // rows,),
        in_specs=[row] * len(pieces),
        out_specs=row,
        out_shape=jax.ShapeDtypeStruct((height, width), BF16),
        compiler_params=params(60),
        cost_estimate=pl.CostEstimate(
            flops=9 * height * width, bytes_accessed=18 * height * width, transcendentals=0
        ),
        name="add",
    )(*pieces)


def epilogue_kernel(
    groups, recv_ref, cot_ref, up_slope_ref, val_slope_ref, act_ref, inv_ref, gain_ref, up_ref, val_ref
):
    rows = cot_ref.shape[0]

    def first(g, dots):
        at = pl.ds(pl.multiple_of(g * LANES, LANES), LANES)
        mid = (cot_ref[:, at].astype(F32) * recv_ref[g, 0].astype(F32)).astype(BF16)
        up_ref[:, at] = (mid.astype(F32) * up_slope_ref[:, at].astype(F32)).astype(BF16)
        scaled = recv_ref[g, 1].astype(F32) * gain_ref[:, at]
        return dots + scaled * act_ref[:, at].astype(F32)

    dots = lax.fori_loop(0, groups, first, jnp.zeros((rows, LANES), F32), unroll=2)
    mean = jnp.sum(dots, axis=1, keepdims=True) * (1.0 / (groups * LANES))
    inv = inv_ref[...]
    pull = inv * inv * inv * mean

    def second(g, carry):
        at = pl.ds(pl.multiple_of(g * LANES, LANES), LANES)
        scaled = recv_ref[g, 1].astype(F32) * gain_ref[:, at]
        slope = inv * scaled - pull * act_ref[:, at].astype(F32)
        val_ref[:, at] = (slope * val_slope_ref[:, at].astype(F32)).astype(BF16)
        return carry

    lax.fori_loop(0, groups, second, 0, unroll=4)


def epilogue(recv, cot, up_slope, val_slope, act, inv, gain, rows=32):
    toks, width = cot.shape
    groups = width // LANES
    row = pl.BlockSpec((rows, width), lambda i: (i, 0))
    out = jax.ShapeDtypeStruct((toks, width), BF16)
    return pl.pallas_call(
        functools.partial(epilogue_kernel, groups),
        grid=(toks // rows,),
        in_specs=[
            pl.BlockSpec((groups, 2, rows, LANES), lambda i: (0, 0, i, 0)),
            row,
            row,
            row,
            row,
            pl.BlockSpec((rows, LANES), lambda i: (i, 0)),
            pl.BlockSpec((1, width), lambda i: (0, 0)),
        ],
        out_specs=[row, row],
        out_shape=[out, out],
        compiler_params=params(60),
        cost_estimate=pl.CostEstimate(
            flops=20 * toks * width, bytes_accessed=22 * toks * width, transcendentals=0
        ),
        name="epilogue",
    )(recv, cot, up_slope, val_slope, act, inv, gain)


def pack_kernel(seqs, parts, sums_ref, out_ref):
    out_ref[...] = jnp.zeros_like(out_ref)
    for a in range(seqs):
        at = slice((a + 1) * LANES, (a + 2) * LANES)
        for y in range(parts):
            out_ref[a * parts + y, :1] = sums_ref[:, :LANES]
            out_ref[a * parts + y, 1:2] = sums_ref[:, at]


def pack(sums, seqs, parts):
    shape = (seqs * parts, 8, LANES)
    return pl.pallas_call(
        functools.partial(pack_kernel, seqs, parts),
        grid=(1,),
        in_specs=[pl.BlockSpec(sums.shape, lambda i: (0, 0))],
        out_specs=pl.BlockSpec(shape, lambda i: (0, 0, 0)),
        out_shape=jax.ShapeDtypeStruct(shape, F32),
        compiler_params=params(60),
        name="pack",
    )(sums)


def shards(cotangent, up_pre, value_pre, spatial_weight, spatial_bias, value_gain):
    planes = lax.axis_size(Z)
    seqs = lax.axis_size(DP)
    parts = lax.axis_size("sp_1")
    block = spatial_weight.shape[2]
    cot, up, val = cotangent[0], up_pre[0], value_pre[0]
    gain = value_gain[None]
    away = [(z * seqs + a, (z ^ a) * seqs + z) for z in range(planes) for a in range(seqs)]
    home = [(there, here) for here, there in away]

    def exchange(x):
        return lax.all_to_all(x, PLANE, split_axis=0, concat_axis=0, tiled=True)

    def across(x, d):
        return lax.ppermute(x, Z, [(z, z ^ d) for z in range(planes)])

    weights = lax.ppermute(spatial_weight[0], Z_DP, away)
    sent, inv = prologue(cot, up, val, gain)
    recv = exchange(sent)
    pieces = [weights] + [across(weights, d) for d in range(1, planes)]
    bias = lax.ppermute(spatial_bias, Z_DP, away)
    bias = jnp.broadcast_to(bias.reshape(block, 1), (block, LANES))
    up_slope, val_slope, act = slopes(up, val)
    back, sums = mix(recv, pieces, bias, seqs, parts)
    back = exchange(back)
    grads = weight_grads(recv, seqs, parts)
    grads = [grads[0]] + [across(grads[d], d) for d in range(1, planes)]
    grads = add(grads)
    sums = lax.psum(sums, Z)
    grads = lax.ppermute(grads, Z_DP, home)
    small = pack(sums, seqs, parts)
    small = exchange(small)
    gain_grad = small[:, 0].reshape(-1) / value_gain
    mine = lax.axis_index(Z) * parts + lax.axis_index("sp_1")
    bias_grad = lax.dynamic_slice_in_dim(small, mine, 1, axis=0)[:, 1]
    up_grad, value_grad = epilogue(back, cot, up_slope, val_slope, act, inv, gain)
    return (up_grad[None], value_grad[None], grads[None].astype(F32), bias_grad, gain_grad)


def solution(mesh):
    torus = Mesh(mesh.devices.reshape(8, 4, 4, 2), ("sp_0", "sp_1", "dp_0", "dp_1"))
    in_specs = (
        P(DP, SP, None),
        P(DP, SP, None),
        P(DP, SP, None),
        P(SP, DP, None),
        P(SP, None),
        P(),
    )
    out_specs = (P(DP, SP, None), P(DP, SP, None), P(SP, DP, None), P(SP, DP), P())
    return jax.shard_map(
        shards, mesh=torus, in_specs=in_specs, out_specs=out_specs, check_vma=False
    )
```

```python
import functools
import math

import jax
import jax.numpy as jnp
from jax import lax
from jax.experimental import pallas as pl
from jax.experimental.pallas import tpu as pltpu
from jax.sharding import Mesh
from jax.sharding import PartitionSpec as P

Z = "sp_0"
SP = ("sp_0", "sp_1")
DP = ("dp_0", "dp_1")
PLANE = ("dp_0", "dp_1", "sp_1")
Z_DP = ("sp_0", "dp_0", "dp_1")

norm_floor = 0.5
root_half = 1.0 / math.sqrt(2.0)
inv_root_tau = 1.0 / math.sqrt(2.0 * math.pi)
LANES = 128
F32 = jnp.float32
BF16 = jnp.bfloat16


def normal_cdf(x):
    return 0.5 * (1.0 + lax.erf(x * root_half))


def params(mib):
    return pltpu.CompilerParams(
        dimension_semantics=("arbitrary",), vmem_limit_bytes=mib * 1024 * 1024
    )


def prologue_kernel(groups, cot_ref, up_ref, val_ref, gain_ref, out_ref, inv_ref, act_ref):
    rows = cot_ref.shape[0]

    def first(g, squares):
        at = pl.ds(pl.multiple_of(g * LANES, LANES), LANES)
        up = up_ref[:, at].astype(F32)
        up_act = (up * normal_cdf(up)).astype(BF16).astype(F32)
        out_ref[g, 0] = (cot_ref[:, at].astype(F32) * up_act).astype(BF16)
        val = val_ref[:, at].astype(F32)
        act = val * normal_cdf(val)
        act_ref[:, at] = act
        return squares + act * act

    squares = lax.fori_loop(0, groups, first, jnp.zeros((rows, LANES), F32), unroll=2)
    mean = jnp.sum(squares, axis=1, keepdims=True) * (1.0 / (groups * LANES))
    inv = lax.rsqrt(mean + norm_floor)
    inv_ref[...] = jnp.broadcast_to(inv, (rows, LANES))

    def second(g, carry):
        at = pl.ds(pl.multiple_of(g * LANES, LANES), LANES)
        out_ref[g, 1] = (act_ref[:, at] * inv * gain_ref[:, at]).astype(BF16)
        return carry

    lax.fori_loop(0, groups, second, 0, unroll=4)


def prologue(cot, up, val, gain, rows=32):
    toks, width = cot.shape
    groups = width // LANES
    row = pl.BlockSpec((rows, width), lambda i: (i, 0))
    return pl.pallas_call(
        functools.partial(prologue_kernel, groups),
        grid=(toks // rows,),
        in_specs=[row, row, row, pl.BlockSpec((1, width), lambda i: (0, 0))],
        out_specs=[
            pl.BlockSpec((groups, 2, rows, LANES), lambda i: (0, 0, i, 0)),
            pl.BlockSpec((rows, LANES), lambda i: (i, 0)),
        ],
        out_shape=[
            jax.ShapeDtypeStruct((groups, 2, toks, LANES), BF16),
            jax.ShapeDtypeStruct((toks, LANES), F32),
        ],
        scratch_shapes=[pltpu.VMEM((rows, width), F32)],
        compiler_params=params(60),
        cost_estimate=pl.CostEstimate(
            flops=100 * toks * width, bytes_accessed=10 * toks * width, transcendentals=0
        ),
        name="prologue",
    )(cot, up, val, gain)


def slopes_kernel(up_ref, val_ref, up_slope_ref, val_slope_ref, act_ref):
    groups = up_ref.shape[1] // LANES

    def step(g, carry):
        at = pl.ds(pl.multiple_of(g * LANES, LANES), LANES)
        up = up_ref[:, at].astype(F32)
        up_slope = normal_cdf(up) + up * (jnp.exp(-0.5 * up * up) * inv_root_tau)
        up_slope_ref[:, at] = up_slope.astype(BF16)
        val = val_ref[:, at].astype(F32)
        phi = normal_cdf(val)
        act_ref[:, at] = (val * phi).astype(BF16)
        val_slope = phi + val * (jnp.exp(-0.5 * val * val) * inv_root_tau)
        val_slope_ref[:, at] = val_slope.astype(BF16)
        return carry

    lax.fori_loop(0, groups, step, 0, unroll=2)


def slopes(up, val, rows=32):
    toks, width = up.shape
    row = pl.BlockSpec((rows, width), lambda i: (i, 0))
    out = jax.ShapeDtypeStruct((toks, width), BF16)
    return pl.pallas_call(
        slopes_kernel,
        grid=(toks // rows,),
        in_specs=[row, row],
        out_specs=[row, row, row],
        out_shape=[out, out, out],
        compiler_params=params(60),
        cost_estimate=pl.CostEstimate(
            flops=100 * toks * width, bytes_accessed=16 * toks * width, transcendentals=0
        ),
        name="slopes",
    )(up, val)


def slab_of(z_offset):
    z = (lax.axis_index(Z) + z_offset + 8) % 8
    return z ^ (lax.axis_index("dp_0") * 2 + lax.axis_index("dp_1"))


ANY = pl.BlockSpec(memory_space=pl.ANY)
VMEM = pl.BlockSpec(memory_space=pltpu.VMEM)
OFFSETS = (0, -1, -2, -3, 1, 2, 3, 4)
PAD = 8


def mix_kernel(seqs, parts, *refs):
    recv_ref, *w_refs = refs[: 1 + seqs]
    bias_ref, out_ref, sums_ref, gate_ref, value_ref, w_ref, mixed_ref, back_ref, sems = refs[1 + seqs :]
    toks = recv_ref.shape[2]
    block = parts * toks
    slab = block // seqs
    pair = 2 * LANES
    steps = seqs // 2

    def columns(j):
        return slice(j * pair, (j + 1) * pair)

    def fetch(which, to_ref, j):
        for b in (2 * j, 2 * j + 1):
            pltpu.make_async_copy(
                recv_ref.at[b * parts : (b + 1) * parts, which],
                to_ref.at[:, :, b * LANES : (b + 1) * LANES],
                sems.at[which, j],
            ).start()

    def fetched(which, to_ref, j):
        part = to_ref.at[:, :, columns(j)]
        pltpu.make_async_copy(part, part, sems.at[which, j]).wait()

    def put(which, from_ref, j):
        for b in (2 * j, 2 * j + 1):
            pltpu.make_async_copy(
                from_ref.at[:, :, b * LANES : (b + 1) * LANES],
                out_ref.at[b, :, which],
                sems.at[2 + which, j],
            ).start()

    for d in range(seqs):
        rows = pl.ds(pl.multiple_of(slab_of(OFFSETS[d]) * slab, slab), slab)
        pltpu.make_async_copy(w_refs[d], w_ref.at[rows], sems.at[4, 0]).start()
    for j in range(steps):
        fetch(0, gate_ref, j)
        fetch(1, value_ref, j)
    bias_col = jnp.transpose(jnp.broadcast_to(bias_ref[...], (8, block)))[:, :1]
    pltpu.make_async_copy(w_ref, w_ref, sems.at[4, 0]).wait()
    sums = jnp.zeros((8, block), F32)
    total = jnp.zeros((8, LANES), F32)
    for j in range(steps):
        fetched(0, gate_ref, j)
        gate = gate_ref[:, :, columns(j)].reshape(block, pair)
        back = lax.dot_general(
            w_ref[...], gate, (((0,), (0,)), ((), ())), preferred_element_type=F32
        ).astype(BF16)
        back_ref[:, :, columns(j)] = back.reshape(parts, toks, pair)
        put(1, back_ref, j)
        sums += lax.dot_general(
            jnp.ones((8, pair), BF16), gate, (((1,), (1,)), ((), ())), preferred_element_type=F32
        )
        fetched(1, value_ref, j)
        value = value_ref[:, :, columns(j)].reshape(block, pair)
        mixed = jnp.dot(w_ref[...], value, preferred_element_type=F32)
        mixed_ref[:, :, columns(j)] = (mixed + bias_col).astype(BF16).reshape(parts, toks, pair)
        put(0, mixed_ref, j)
        terms = back.astype(F32) * value.astype(F32)
        terms = jnp.sum(terms.reshape(block // 8, 8, pair), axis=0)
        total += terms[:, :LANES] + terms[:, LANES:]
    sums_ref[:, LANES:] = sums[:1]
    sums_ref[:, :LANES] = jnp.sum(total, axis=0, keepdims=True)
    for which, from_ref in ((1, back_ref), (0, mixed_ref)):
        for j in range(steps):
            part = from_ref.at[:, :, columns(j)]
            pltpu.make_async_copy(part, part, sems.at[2 + which, j]).wait()


def mix(recv, pieces, bias, seqs, parts):
    toks = recv.shape[2]
    block = parts * toks
    flat = pltpu.VMEM((parts, toks, seqs * LANES), BF16)
    out, sums = pl.pallas_call(
        functools.partial(mix_kernel, seqs, parts),
        in_specs=[ANY] * (1 + seqs) + [VMEM],
        out_specs=[ANY, VMEM],
        out_shape=[
            jax.ShapeDtypeStruct((seqs, parts, 2, toks, LANES), BF16),
            jax.ShapeDtypeStruct((1, LANES + block), F32),
        ],
        scratch_shapes=[
            flat,
            flat,
            pltpu.VMEM((block, block), BF16),
            flat,
            flat,
            pltpu.SemaphoreType.DMA((5, seqs // 2)),
        ],
        compiler_params=pltpu.CompilerParams(vmem_limit_bytes=60 * 1024 * 1024),
        cost_estimate=pl.CostEstimate(
            flops=4 * block * block * seqs * LANES, bytes_accessed=10 * block * block, transcendentals=0
        ),
        name="mix",
    )(recv, *pieces, bias)
    return out.reshape(recv.shape), sums


def split(x):
    high = x.astype(BF16)
    middle = (x - high.astype(F32)).astype(BF16)
    low = (x - high.astype(F32) - middle.astype(F32)).astype(BF16)
    return high, middle, low


def pack_sums(sums):
    bias = split(sums[:, LANES:])
    wide = jnp.concatenate([sums[:, :LANES], jnp.zeros_like(sums[:, 2 * LANES :])], axis=1)
    gain = split(wide)
    zeros = jnp.zeros_like(bias[0])
    return jnp.concatenate([*bias, *gain, zeros, zeros], axis=0)


def unpack_sums(rows):
    rows = rows.astype(F32)
    bias = rows[0:1] + rows[1:2] + rows[2:3]
    gain = rows[3:4] + rows[4:5] + rows[5:6]
    return jnp.concatenate([gain[:, :LANES], bias], axis=1)


def grads_kernel(seqs, parts, recv_ref, sums_ref, *refs):
    outs = refs[:seqs]
    gate_ref, value_ref, grad_ref, rows_ref, sems = refs[seqs:]
    toks = recv_ref.shape[2]
    block = parts * toks
    slab = block // seqs
    for b in range(seqs):
        cols = slice(b * LANES, (b + 1) * LANES)
        pieces = slice(b * parts, (b + 1) * parts)
        pltpu.make_async_copy(recv_ref.at[pieces, 0], gate_ref.at[:, :, cols], sems.at[0, 0]).start()
        pltpu.make_async_copy(recv_ref.at[pieces, 1], value_ref.at[:, :, cols], sems.at[1, 0]).start()
    rows_ref[...] = pack_sums(sums_ref[...])
    for d in range(seqs):
        pltpu.make_async_copy(rows_ref, outs[d].at[slab:], sems.at[3, d]).start()
    pltpu.make_async_copy(gate_ref, gate_ref, sems.at[0, 0]).wait()
    pltpu.make_async_copy(value_ref, value_ref, sems.at[1, 0]).wait()

    def step(y, carry):
        grad = lax.dot_general(
            gate_ref[...].reshape(block, seqs * LANES),
            value_ref[y],
            (((1,), (1,)), ((), ())),
            preferred_element_type=F32,
        )
        grad_ref[y] = grad.astype(BF16)
        at = pl.ds(pl.multiple_of(y * toks, toks), toks)
        for d in range(seqs):
            rows = pl.ds(pl.multiple_of(slab_of(-OFFSETS[d]) * slab, slab), slab)
            pltpu.make_async_copy(grad_ref.at[y, rows], outs[d].at[:slab, at], sems.at[2, 0]).start()
        return carry

    lax.fori_loop(0, parts, step, 0)
    pltpu.make_async_copy(grad_ref, grad_ref, sems.at[2, 0]).wait()
    for d in range(seqs):
        pltpu.make_async_copy(rows_ref, outs[d].at[slab:], sems.at[3, d]).wait()


def weight_grads(recv, sums, seqs, parts):
    toks = recv.shape[2]
    block = parts * toks
    flat = pltpu.VMEM((parts, toks, seqs * LANES), BF16)
    return pl.pallas_call(
        functools.partial(grads_kernel, seqs, parts),
        in_specs=[ANY, VMEM],
        out_specs=[ANY] * seqs,
        out_shape=[jax.ShapeDtypeStruct((block // seqs + PAD, block), BF16)] * seqs,
        scratch_shapes=[
            flat,
            flat,
            pltpu.VMEM((parts, block, toks), BF16),
            pltpu.VMEM((PAD, block), BF16),
            pltpu.SemaphoreType.DMA((4, seqs)),
        ],
        compiler_params=pltpu.CompilerParams(vmem_limit_bytes=60 * 1024 * 1024),
        cost_estimate=pl.CostEstimate(
            flops=2 * block * block * seqs * LANES, bytes_accessed=6 * block * block, transcendentals=0
        ),
        name="weight_grads",
    )(recv, sums)


def hop_kernel(slab, *refs):
    n = len(refs) // 3
    for here, there, out in zip(refs[:n], refs[n : 2 * n], refs[2 * n :]):
        out[:slab] = (here[:slab].astype(F32) + there[:slab].astype(F32)).astype(BF16)
        out[slab:] = pack_sums(unpack_sums(here[slab:]) + unpack_sums(there[slab:]))


def hop(here, there):
    height, width = here[0].shape
    return pl.pallas_call(
        functools.partial(hop_kernel, height - PAD),
        in_specs=[VMEM] * (2 * len(here)),
        out_specs=[VMEM] * len(here),
        out_shape=[jax.ShapeDtypeStruct((height, width), BF16)] * len(here),
        compiler_params=pltpu.CompilerParams(vmem_limit_bytes=8 * 1024 * 1024),
        cost_estimate=pl.CostEstimate(
            flops=2 * height * width, bytes_accessed=12 * height * width, transcendentals=0
        ),
        name="hop",
    )(*here, *there)


def last_kernel(slab, *refs):
    *ins, grad_ref = refs
    grad_ref[...] = sum(r[:slab].astype(F32) for r in ins).astype(BF16)


def last(pieces):
    height, width = pieces[0].shape
    return pl.pallas_call(
        functools.partial(last_kernel, height - PAD),
        in_specs=[VMEM] * 3,
        out_specs=VMEM,
        out_shape=jax.ShapeDtypeStruct((height - PAD, width), BF16),
        compiler_params=pltpu.CompilerParams(vmem_limit_bytes=8 * 1024 * 1024),
        cost_estimate=pl.CostEstimate(
            flops=4 * height * width, bytes_accessed=8 * height * width, transcendentals=0
        ),
        name="last",
    )(*pieces)


def pack_kernel(slab, seqs, parts, *refs):
    *ins, small_ref = refs
    sums = sum(unpack_sums(r[slab:]) for r in ins)
    small_ref[...] = jnp.zeros_like(small_ref)
    for a in range(seqs):
        at = slice((a + 1) * LANES, (a + 2) * LANES)
        for y in range(parts):
            small_ref[a * parts + y, :1] = sums[:, :LANES]
            small_ref[a * parts + y, 1:2] = sums[:, at]


def pack(pieces, seqs, parts):
    slab = pieces[0].shape[0] - PAD
    return pl.pallas_call(
        functools.partial(pack_kernel, slab, seqs, parts),
        in_specs=[VMEM] * 3,
        out_specs=VMEM,
        out_shape=jax.ShapeDtypeStruct((seqs * parts, 8, LANES), F32),
        compiler_params=pltpu.CompilerParams(vmem_limit_bytes=8 * 1024 * 1024),
        name="pack",
    )(*pieces)


def epilogue_kernel(
    groups, recv_ref, cot_ref, up_slope_ref, val_slope_ref, act_ref, inv_ref, gain_ref, up_ref, val_ref
):
    rows = cot_ref.shape[0]

    def first(g, dots):
        at = pl.ds(pl.multiple_of(g * LANES, LANES), LANES)
        mid = (cot_ref[:, at].astype(F32) * recv_ref[g, 0].astype(F32)).astype(BF16)
        up_ref[:, at] = (mid.astype(F32) * up_slope_ref[:, at].astype(F32)).astype(BF16)
        scaled = recv_ref[g, 1].astype(F32) * gain_ref[:, at]
        return dots + scaled * act_ref[:, at].astype(F32)

    dots = lax.fori_loop(0, groups, first, jnp.zeros((rows, LANES), F32), unroll=2)
    mean = jnp.sum(dots, axis=1, keepdims=True) * (1.0 / (groups * LANES))
    inv = inv_ref[...]
    pull = inv * inv * inv * mean

    def second(g, carry):
        at = pl.ds(pl.multiple_of(g * LANES, LANES), LANES)
        scaled = recv_ref[g, 1].astype(F32) * gain_ref[:, at]
        slope = inv * scaled - pull * act_ref[:, at].astype(F32)
        val_ref[:, at] = (slope * val_slope_ref[:, at].astype(F32)).astype(BF16)
        return carry

    lax.fori_loop(0, groups, second, 0, unroll=4)


def epilogue(recv, cot, up_slope, val_slope, act, inv, gain, rows=32):
    toks, width = cot.shape
    groups = width // LANES
    row = pl.BlockSpec((rows, width), lambda i: (i, 0))
    out = jax.ShapeDtypeStruct((toks, width), BF16)
    return pl.pallas_call(
        functools.partial(epilogue_kernel, groups),
        grid=(toks // rows,),
        in_specs=[
            pl.BlockSpec((groups, 2, rows, LANES), lambda i: (0, 0, i, 0)),
            row,
            row,
            row,
            row,
            pl.BlockSpec((rows, LANES), lambda i: (i, 0)),
            pl.BlockSpec((1, width), lambda i: (0, 0)),
        ],
        out_specs=[row, row],
        out_shape=[out, out],
        compiler_params=params(60),
        cost_estimate=pl.CostEstimate(
            flops=20 * toks * width, bytes_accessed=22 * toks * width, transcendentals=0
        ),
        name="epilogue",
    )(recv, cot, up_slope, val_slope, act, inv, gain)


def shards(cotangent, up_pre, value_pre, spatial_weight, spatial_bias, value_gain):
    planes = lax.axis_size(Z)
    seqs = lax.axis_size(DP)
    parts = lax.axis_size("sp_1")
    cot, up, val = cotangent[0], up_pre[0], value_pre[0]
    gain = value_gain[None]
    away = [(z * seqs + a, (z ^ a) * seqs + z) for z in range(planes) for a in range(seqs)]
    home = [(there, here) for here, there in away]

    def exchange(x):
        return lax.all_to_all(x, PLANE, split_axis=0, concat_axis=0, tiled=True)

    def shifted(x, by):
        return lax.ppermute(x, Z, [(z, (z + by) % planes) for z in range(planes)])

    weights = lax.ppermute(spatial_weight[0], Z_DP, away)
    bias = lax.ppermute(spatial_bias, Z_DP, away)
    sent, inv = prologue(cot, up, val, gain)
    recv = exchange(sent)
    before, after = [weights], [weights]
    for _ in range(3):
        before.append(shifted(before[-1], 1))
        after.append(shifted(after[-1], -1))
    after.append(shifted(after[-1], -1))
    pieces = before + after[1:]
    up_slope, val_slope, act = slopes(up, val)
    back, sums = mix(recv, pieces, bias, seqs, parts)
    back = exchange(back)
    own, p1, p2, p3, m1, m2, m3, m4 = weight_grads(recv, sums, seqs, parts)
    plus, minus = shifted(p3, 1), shifted(m4, -1)
    plus, minus = hop((p2, m3), (plus, minus))
    plus, minus = shifted(plus, 1), shifted(minus, -1)
    plus, minus = hop((p1, m2), (plus, minus))
    plus, minus = shifted(plus, 1), shifted(minus, -1)
    (minus,) = hop((m1,), (minus,))
    minus = shifted(minus, -1)
    grads = last((own, plus, minus))
    grads = lax.ppermute(grads, Z_DP, home)
    small = pack((own, plus, minus), seqs, parts)
    small = exchange(small)
    gain_grad = small[:, 0].reshape(-1) / value_gain
    mine = lax.axis_index(Z) * parts + lax.axis_index("sp_1")
    bias_grad = lax.dynamic_slice_in_dim(small, mine, 1, axis=0)[:, 1]
    up_grad, value_grad = epilogue(back, cot, up_slope, val_slope, act, inv, gain)
    return (up_grad[None], value_grad[None], grads[None].astype(F32), bias_grad, gain_grad)


def solution(mesh):
    torus = Mesh(mesh.devices.reshape(8, 4, 4, 2), ("sp_0", "sp_1", "dp_0", "dp_1"))
    in_specs = (
        P(DP, SP, None),
        P(DP, SP, None),
        P(DP, SP, None),
        P(SP, DP, None),
        P(SP, None),
        P(),
    )
    out_specs = (P(DP, SP, None), P(DP, SP, None), P(SP, DP, None), P(SP, DP), P())
    return jax.shard_map(
        shards, mesh=torus, in_specs=in_specs, out_specs=out_specs, check_vma=False
    )
```

```python
import functools
import math

import jax
import jax.numpy as jnp
from jax import lax
from jax.experimental import pallas as pl
from jax.experimental.pallas import tpu as pltpu
from jax.sharding import Mesh
from jax.sharding import PartitionSpec as P

Z = "sp_0"
SP = ("sp_0", "sp_1")
DP = ("dp_0", "dp_1")
PLANE = ("dp_0", "dp_1", "sp_1")
Z_DP = ("sp_0", "dp_0", "dp_1")

norm_floor = 0.5
root_half = 1.0 / math.sqrt(2.0)
inv_root_tau = 1.0 / math.sqrt(2.0 * math.pi)
LANES = 128
F32 = jnp.float32
BF16 = jnp.bfloat16


def normal_cdf(x):
    return 0.5 * (1.0 + lax.erf(x * root_half))


HBM = pl.BlockSpec(memory_space=pltpu.HBM)
VMEM = pl.BlockSpec(memory_space=pltpu.VMEM)


def limit(mib):
    return pltpu.CompilerParams(vmem_limit_bytes=mib * 1024 * 1024)


def params(mib):
    return pltpu.CompilerParams(
        dimension_semantics=("arbitrary",), vmem_limit_bytes=mib * 1024 * 1024
    )


def prologue_kernel(
    groups, rows, cot_hbm, up_hbm, val_hbm, gain_ref, out_hbm, inv_ref, cot_ref, up_ref, val_ref, out_ref, act_ref, sems
):
    toks = cot_ref.shape[0]
    steps = toks // rows

    def loads(i):
        at = pl.ds(pl.multiple_of(i * rows, rows), rows)
        pairs = ((cot_hbm, cot_ref), (up_hbm, up_ref), (val_hbm, val_ref))
        return [
            pltpu.make_async_copy(src.at[at], dst.at[at], sems.at[k, i])
            for k, (src, dst) in enumerate(pairs)
        ]

    def store(i):
        at = pl.ds(pl.multiple_of(i * rows, rows), rows)
        return pltpu.make_async_copy(out_ref.at[:, :, at], out_hbm.at[:, :, at], sems.at[3, i])

    for i in range(AHEAD):
        for copy in loads(i):
            copy.start()

    def step(i, carry):
        for copy in loads(i):
            copy.wait()

        @pl.when(i + AHEAD < steps)
        def _():
            for copy in loads(i + AHEAD):
                copy.start()

        at = pl.ds(pl.multiple_of(i * rows, rows), rows)

        def first(g, squares):
            cols = pl.ds(pl.multiple_of(g * LANES, LANES), LANES)
            up = up_ref[at, cols].astype(F32)
            up_act = (up * normal_cdf(up)).astype(BF16).astype(F32)
            out_ref[g, 0, at] = (cot_ref[at, cols].astype(F32) * up_act).astype(BF16)
            val = val_ref[at, cols].astype(F32)
            act = val * normal_cdf(val)
            act_ref[:, cols] = act
            return squares + act * act

        squares = lax.fori_loop(0, groups, first, jnp.zeros((rows, LANES), F32), unroll=UNROLL)
        mean = jnp.sum(squares, axis=1, keepdims=True) * (1.0 / (groups * LANES))
        inv = lax.rsqrt(mean + norm_floor)
        inv_ref[at] = jnp.broadcast_to(inv, (rows, LANES))

        def second(g, carry):
            cols = pl.ds(pl.multiple_of(g * LANES, LANES), LANES)
            out_ref[g, 1, at] = (act_ref[:, cols] * inv * gain_ref[:, cols]).astype(BF16)
            return carry

        lax.fori_loop(0, groups, second, 0, unroll=4)
        store(i).start()
        return carry

    lax.fori_loop(0, steps, step, 0)
    for i in range(steps):
        store(i).wait()


UNROLL = 4
AHEAD = 4


def prologue(cot, up, val, gain, rows=64):
    toks, width = cot.shape
    groups = width // LANES
    whole = pltpu.VMEM((toks, width), BF16)
    return pl.pallas_call(
        functools.partial(prologue_kernel, groups, rows),
        in_specs=[HBM, HBM, HBM, VMEM],
        out_specs=[HBM, VMEM],
        out_shape=[
            jax.ShapeDtypeStruct((groups, 2, toks, LANES), BF16),
            jax.ShapeDtypeStruct((toks, LANES), F32),
        ],
        scratch_shapes=[
            whole,
            whole,
            whole,
            pltpu.VMEM((groups, 2, toks, LANES), BF16),
            pltpu.VMEM((rows, width), F32),
            pltpu.SemaphoreType.DMA((4, toks // rows)),
        ],
        compiler_params=limit(60),
        cost_estimate=pl.CostEstimate(
            flops=100 * toks * width, bytes_accessed=10 * toks * width, transcendentals=0
        ),
        name="prologue",
    )(cot, up, val, gain)


def slopes_kernel(up_ref, val_ref, up_slope_ref, val_slope_ref, act_ref):
    groups = up_ref.shape[1] // LANES

    def step(g, carry):
        at = pl.ds(pl.multiple_of(g * LANES, LANES), LANES)
        up = up_ref[:, at].astype(F32)
        up_slope = normal_cdf(up) + up * (jnp.exp(-0.5 * up * up) * inv_root_tau)
        up_slope_ref[:, at] = up_slope.astype(BF16)
        val = val_ref[:, at].astype(F32)
        phi = normal_cdf(val)
        act_ref[:, at] = (val * phi).astype(BF16)
        val_slope = phi + val * (jnp.exp(-0.5 * val * val) * inv_root_tau)
        val_slope_ref[:, at] = val_slope.astype(BF16)
        return carry

    lax.fori_loop(0, groups, step, 0, unroll=2)


def slopes(up, val, rows=64):
    toks, width = up.shape
    row = pl.BlockSpec((rows, width), lambda i: (i, 0))
    out = jax.ShapeDtypeStruct((toks, width), BF16)
    return pl.pallas_call(
        slopes_kernel,
        grid=(toks // rows,),
        in_specs=[row, row],
        out_specs=[row, row, row],
        out_shape=[out, out, out],
        compiler_params=params(60),
        cost_estimate=pl.CostEstimate(
            flops=100 * toks * width, bytes_accessed=16 * toks * width, transcendentals=0
        ),
        name="slopes",
    )(up, val)


def slab_of(z_offset):
    z = (lax.axis_index(Z) + z_offset + 8) % 8
    return z ^ (lax.axis_index("dp_0") * 2 + lax.axis_index("dp_1"))


OFFSETS = (0, -1, -2, -3, 1, 2, 3, 4)
PAD = 8


def arrange_kernel(*refs):
    *pieces, w_ref, wt_ref = refs
    slab = pieces[0].shape[0]
    for d, piece in enumerate(pieces):
        at = pl.ds(pl.multiple_of(slab_of(OFFSETS[d]) * slab, slab), slab)
        rows = piece[...]
        w_ref[at] = rows
        wt_ref[:, at] = jnp.transpose(rows)


def arrange(pieces):
    _, block = pieces[0].shape
    return pl.pallas_call(
        arrange_kernel,
        in_specs=[VMEM] * len(pieces),
        out_specs=[VMEM] * 2,
        out_shape=[
            jax.ShapeDtypeStruct((block, block), BF16),
            jax.ShapeDtypeStruct((block, block), BF16),
        ],
        compiler_params=limit(8),
        cost_estimate=pl.CostEstimate(
            flops=4 * block * block, bytes_accessed=6 * block * block, transcendentals=0
        ),
        name="arrange",
    )(*pieces)


def mix_kernel(
    seqs, parts, per, recv_hbm, w_hbm, wt_hbm, bias_row_ref, out_hbm, sums_ref,
    recv_ref, out_ref, w_ref, wt_ref, bias_ref, sems, fixed_sems
):
    toks = recv_ref.shape[2]
    block = parts * toks
    steps = seqs // per

    def load(j):
        at = pl.ds(j * (per * parts), per * parts)
        return pltpu.make_async_copy(recv_hbm.at[at], recv_ref.at[at], sems.at[0, j])

    def store(j):
        at = pl.ds(j * per, per)
        return pltpu.make_async_copy(out_ref.at[at], out_hbm.at[at], sems.at[1, j])

    def side_by_side(j, which):
        return jnp.concatenate(
            [
                recv_ref[pl.ds((j * per + b) * parts, parts), which].reshape(block, LANES)
                for b in range(per)
            ],
            axis=1,
        )

    fixed = [
        pltpu.make_async_copy(src, dst, fixed_sems.at[k])
        for k, (src, dst) in enumerate(((wt_hbm, wt_ref), (w_hbm, w_ref)))
    ]
    fixed[0].start()
    load(0).start()
    fixed[1].start()
    for j in range(1, steps):
        load(j).start()
    bias_ref[...] = jnp.transpose(jnp.broadcast_to(bias_row_ref[...], (LANES, block)))
    fixed[0].wait()

    def step(j, total):
        load(j).wait()
        gate = side_by_side(j, 0)
        back = jnp.dot(wt_ref[...], gate, preferred_element_type=F32).astype(BF16)
        value = side_by_side(j, 1)
        for b in range(per):
            cols = slice(b * LANES, (b + 1) * LANES)
            out_ref[j * per + b, :, 1] = back[:, cols].reshape(parts, toks, LANES)
            terms = back[:, cols].astype(F32) * value[:, cols].astype(F32)
            total += jnp.sum(terms.reshape(block // 8, 8, LANES), axis=0)

        @pl.when(j == 0)
        def _():
            fixed[1].wait()

        mixed = jnp.dot(w_ref[...], value, preferred_element_type=F32)
        for b in range(per):
            cols = slice(b * LANES, (b + 1) * LANES)
            part = (mixed[:, cols] + bias_ref[...]).astype(BF16)
            out_ref[j * per + b, :, 0] = part.reshape(parts, toks, LANES)
        store(j).start()
        return total

    total = lax.fori_loop(0, steps, step, jnp.zeros((8, LANES), F32))
    sums_ref[...] = jnp.sum(total, axis=0, keepdims=True)
    for j in range(steps):
        store(j).wait()


PER = 4


def mix(recv, w, wt, bias, seqs, parts):
    toks = recv.shape[2]
    block = parts * toks
    whole = (seqs, parts, 2, toks, LANES)
    out, sums = pl.pallas_call(
        functools.partial(mix_kernel, seqs, parts, PER),
        in_specs=[HBM] * 3 + [VMEM],
        out_specs=[HBM, VMEM],
        out_shape=[jax.ShapeDtypeStruct(whole, BF16), jax.ShapeDtypeStruct((1, LANES), F32)],
        scratch_shapes=[
            pltpu.VMEM(recv.shape, BF16),
            pltpu.VMEM(whole, BF16),
            pltpu.VMEM((block, block), BF16),
            pltpu.VMEM((block, block), BF16),
            pltpu.VMEM((block, LANES), F32),
            pltpu.SemaphoreType.DMA((2, seqs // PER)),
            pltpu.SemaphoreType.DMA((2,)),
        ],
        compiler_params=limit(60),
        cost_estimate=pl.CostEstimate(
            flops=4 * block * block * seqs * LANES, bytes_accessed=10 * block * block, transcendentals=0
        ),
        name="mix",
    )(recv, w, wt, bias)
    return out.reshape(recv.shape), sums


def split(x):
    high = x.astype(BF16)
    middle = (x - high.astype(F32)).astype(BF16)
    low = (x - high.astype(F32) - middle.astype(F32)).astype(BF16)
    return high, middle, low


def pack_sums(sums):
    bias = split(sums[:, LANES:])
    wide = jnp.concatenate([sums[:, :LANES], jnp.zeros_like(sums[:, 2 * LANES :])], axis=1)
    gain = split(wide)
    zeros = jnp.zeros_like(bias[0])
    return jnp.concatenate([*bias, *gain, zeros, zeros], axis=0)


def unpack_sums(rows):
    rows = rows.astype(F32)
    bias = rows[0:1] + rows[1:2] + rows[2:3]
    gain = rows[3:4] + rows[4:5] + rows[5:6]
    return jnp.concatenate([gain[:, :LANES], bias], axis=1)


def grads_kernel(seqs, parts, recv_ref, sums_ref, *refs):
    outs = refs[:seqs]
    gate_ref, value_ref, grad_ref, rows_ref, sems = refs[seqs:]
    toks = recv_ref.shape[2]
    block = parts * toks
    slab = block // seqs
    for b in range(seqs):
        cols = slice(b * LANES, (b + 1) * LANES)
        pieces = slice(b * parts, (b + 1) * parts)
        pltpu.make_async_copy(recv_ref.at[pieces, 0], gate_ref.at[:, :, cols], sems.at[0, 0]).start()
        pltpu.make_async_copy(recv_ref.at[pieces, 1], value_ref.at[:, :, cols], sems.at[1, 0]).start()
    pltpu.make_async_copy(gate_ref, gate_ref, sems.at[0, 0]).wait()
    bias_sums = []
    for y in range(parts):
        gate = gate_ref[y].astype(F32)
        gate = sum(gate[:, b * LANES : (b + 1) * LANES] for b in range(seqs))
        bias_sums.append(jnp.sum(jnp.transpose(gate), axis=0, keepdims=True))
    rows_ref[...] = pack_sums(jnp.concatenate([sums_ref[...], *bias_sums], axis=1))
    for d in range(seqs):
        pltpu.make_async_copy(rows_ref, outs[d].at[slab:], sems.at[3, d]).start()
    pltpu.make_async_copy(value_ref, value_ref, sems.at[1, 0]).wait()

    def step(y, carry):
        grad = lax.dot_general(
            gate_ref[...].reshape(block, seqs * LANES),
            value_ref[y],
            (((1,), (1,)), ((), ())),
            preferred_element_type=F32,
        )
        grad_ref[y] = grad.astype(BF16)
        at = pl.ds(pl.multiple_of(y * toks, toks), toks)
        for d in range(seqs):
            rows = pl.ds(pl.multiple_of(slab_of(-OFFSETS[d]) * slab, slab), slab)
            pltpu.make_async_copy(grad_ref.at[y, rows], outs[d].at[:slab, at], sems.at[2, 0]).start()
        return carry

    lax.fori_loop(0, parts, step, 0)
    pltpu.make_async_copy(grad_ref, grad_ref, sems.at[2, 0]).wait()
    for d in range(seqs):
        pltpu.make_async_copy(rows_ref, outs[d].at[slab:], sems.at[3, d]).wait()


def weight_grads(recv, sums, seqs, parts):
    toks = recv.shape[2]
    block = parts * toks
    flat = pltpu.VMEM((parts, toks, seqs * LANES), BF16)
    return pl.pallas_call(
        functools.partial(grads_kernel, seqs, parts),
        in_specs=[HBM, VMEM],
        out_specs=[HBM] * seqs,
        out_shape=[jax.ShapeDtypeStruct((block // seqs + PAD, block), BF16)] * seqs,
        scratch_shapes=[
            flat,
            flat,
            pltpu.VMEM((parts, block, toks), BF16),
            pltpu.VMEM((PAD, block), BF16),
            pltpu.SemaphoreType.DMA((4, seqs)),
        ],
        compiler_params=limit(28),
        cost_estimate=pl.CostEstimate(
            flops=2 * block * block * seqs * LANES, bytes_accessed=6 * block * block, transcendentals=0
        ),
        name="weight_grads",
    )(recv, sums)


def hop_kernel(slab, *refs):
    n = len(refs) // 3
    for here, there, out in zip(refs[:n], refs[n : 2 * n], refs[2 * n :]):
        out[:slab] = (here[:slab].astype(F32) + there[:slab].astype(F32)).astype(BF16)
        out[slab:] = pack_sums(unpack_sums(here[slab:]) + unpack_sums(there[slab:]))


def hop(here, there):
    height, width = here[0].shape
    return pl.pallas_call(
        functools.partial(hop_kernel, height - PAD),
        in_specs=[VMEM] * (2 * len(here)),
        out_specs=[VMEM] * len(here),
        out_shape=[jax.ShapeDtypeStruct((height, width), BF16)] * len(here),
        compiler_params=limit(8),
        cost_estimate=pl.CostEstimate(
            flops=2 * height * width, bytes_accessed=12 * height * width, transcendentals=0
        ),
        name="hop",
    )(*here, *there)


def last_kernel(slab, *refs):
    *ins, grad_ref = refs
    grad_ref[...] = sum(r[:slab].astype(F32) for r in ins).astype(BF16)


def last(pieces):
    height, width = pieces[0].shape
    return pl.pallas_call(
        functools.partial(last_kernel, height - PAD),
        in_specs=[VMEM] * 3,
        out_specs=VMEM,
        out_shape=jax.ShapeDtypeStruct((height - PAD, width), BF16),
        compiler_params=limit(8),
        cost_estimate=pl.CostEstimate(
            flops=4 * height * width, bytes_accessed=8 * height * width, transcendentals=0
        ),
        name="last",
    )(*pieces)


def pack_kernel(slab, seqs, parts, *refs):
    *ins, small_ref = refs
    sums = sum(unpack_sums(r[slab:]) for r in ins)
    small_ref[...] = jnp.zeros_like(small_ref)
    for a in range(seqs):
        at = slice((a + 1) * LANES, (a + 2) * LANES)
        for y in range(parts):
            small_ref[a * parts + y, :1] = sums[:, :LANES]
            small_ref[a * parts + y, 1:2] = sums[:, at]


def pack(pieces, seqs, parts):
    slab = pieces[0].shape[0] - PAD
    return pl.pallas_call(
        functools.partial(pack_kernel, slab, seqs, parts),
        in_specs=[VMEM] * 3,
        out_specs=VMEM,
        out_shape=jax.ShapeDtypeStruct((seqs * parts, 8, LANES), F32),
        compiler_params=limit(8),
        name="pack",
    )(*pieces)


def epilogue_kernel(
    groups, rows, recv_hbm, cot_hbm, up_slope_hbm, val_slope_hbm, act_hbm, inv_ref, gain_ref, up_hbm, val_hbm,
    recv_ref, cot_ref, up_slope_ref, val_slope_ref, act_ref, up_ref, val_ref, sems
):
    toks = cot_ref.shape[0]
    steps = toks // rows

    def loads(i):
        at = pl.ds(pl.multiple_of(i * rows, rows), rows)
        pairs = (
            (cot_hbm, cot_ref),
            (up_slope_hbm, up_slope_ref),
            (val_slope_hbm, val_slope_ref),
            (act_hbm, act_ref),
        )
        return [pltpu.make_async_copy(recv_hbm.at[:, :, at], recv_ref.at[:, :, at], sems.at[0, i])] + [
            pltpu.make_async_copy(src.at[at], dst.at[at], sems.at[3 + k, i])
            for k, (src, dst) in enumerate(pairs)
        ]

    def stores(i):
        at = pl.ds(pl.multiple_of(i * rows, rows), rows)
        return [
            pltpu.make_async_copy(up_ref.at[at], up_hbm.at[at], sems.at[1, i]),
            pltpu.make_async_copy(val_ref.at[at], val_hbm.at[at], sems.at[2, i]),
        ]

    for i in range(AHEAD):
        for copy in loads(i):
            copy.start()

    def step(i, carry):
        for copy in loads(i):
            copy.wait()

        @pl.when(i + AHEAD < steps)
        def _():
            for copy in loads(i + AHEAD):
                copy.start()

        at = pl.ds(pl.multiple_of(i * rows, rows), rows)

        def first(g, dots):
            cols = pl.ds(pl.multiple_of(g * LANES, LANES), LANES)
            mid = (cot_ref[at, cols].astype(F32) * recv_ref[g, 0, at].astype(F32)).astype(BF16)
            up_ref[at, cols] = (mid.astype(F32) * up_slope_ref[at, cols].astype(F32)).astype(BF16)
            scaled = recv_ref[g, 1, at].astype(F32) * gain_ref[:, cols]
            return dots + scaled * act_ref[at, cols].astype(F32)

        dots = lax.fori_loop(0, groups, first, jnp.zeros((rows, LANES), F32), unroll=4)
        mean = jnp.sum(dots, axis=1, keepdims=True) * (1.0 / (groups * LANES))
        inv = inv_ref[at]
        pull = inv * inv * inv * mean

        def second(g, carry):
            cols = pl.ds(pl.multiple_of(g * LANES, LANES), LANES)
            scaled = recv_ref[g, 1, at].astype(F32) * gain_ref[:, cols]
            slope = inv * scaled - pull * act_ref[at, cols].astype(F32)
            val_ref[at, cols] = (slope * val_slope_ref[at, cols].astype(F32)).astype(BF16)
            return carry

        lax.fori_loop(0, groups, second, 0, unroll=4)
        for copy in stores(i):
            copy.start()
        return carry

    lax.fori_loop(0, steps, step, 0)
    for i in range(steps):
        for copy in stores(i):
            copy.wait()


def epilogue(recv, cot, up_slope, val_slope, act, inv, gain, rows=64):
    toks, width = cot.shape
    groups = width // LANES
    out = jax.ShapeDtypeStruct((toks, width), BF16)
    whole = pltpu.VMEM((toks, width), BF16)
    return pl.pallas_call(
        functools.partial(epilogue_kernel, groups, rows),
        in_specs=[HBM] * 5 + [VMEM] * 2,
        out_specs=[HBM, HBM],
        out_shape=[out, out],
        scratch_shapes=[
            pltpu.VMEM(recv.shape, BF16),
            whole,
            whole,
            whole,
            whole,
            whole,
            whole,
            pltpu.SemaphoreType.DMA((7, toks // rows)),
        ],
        compiler_params=limit(EPI_MIB),
        cost_estimate=pl.CostEstimate(
            flops=20 * toks * width, bytes_accessed=22 * toks * width, transcendentals=0
        ),
        name="epilogue",
    )(recv, cot, up_slope, val_slope, act, inv, gain)


EPI_MIB = 60


def shards(cotangent, up_pre, value_pre, spatial_weight, spatial_bias, value_gain):
    planes = lax.axis_size(Z)
    seqs = lax.axis_size(DP)
    parts = lax.axis_size("sp_1")
    cot, up, val = cotangent[0], up_pre[0], value_pre[0]
    gain = value_gain[None]
    away = [(z * seqs + a, (z ^ a) * seqs + z) for z in range(planes) for a in range(seqs)]
    home = [(there, here) for here, there in away]

    def exchange(x):
        return lax.all_to_all(x, PLANE, split_axis=0, concat_axis=0, tiled=True)

    def shifted(x, by):
        return lax.ppermute(x, Z, [(z, (z + by) % planes) for z in range(planes)])

    weights = lax.ppermute(spatial_weight[0], Z_DP, away)
    bias = lax.ppermute(spatial_bias, Z_DP, away)
    sent, inv = prologue(cot, up, val, gain)
    recv = exchange(sent)
    before, after = [weights], [weights]
    for _ in range(3):
        before.append(shifted(before[-1], 1))
        after.append(shifted(after[-1], -1))
    after.append(shifted(after[-1], -1))
    pieces = before + after[1:]
    up_slope, val_slope, act = slopes(up, val)
    w, wt = arrange(pieces)
    back, sums = mix(recv, w, wt, bias, seqs, parts)
    back = exchange(back)
    own, p1, p2, p3, m1, m2, m3, m4 = weight_grads(recv, sums, seqs, parts)
    plus, minus = shifted(p3, 1), shifted(m4, -1)
    plus, minus = hop((p2, m3), (plus, minus))
    plus, minus = shifted(plus, 1), shifted(minus, -1)
    plus, minus = hop((p1, m2), (plus, minus))
    plus, minus = shifted(plus, 1), shifted(minus, -1)
    (minus,) = hop((m1,), (minus,))
    minus = shifted(minus, -1)
    grads = last((own, plus, minus))
    grads = lax.ppermute(grads, Z_DP, home)
    small = pack((own, plus, minus), seqs, parts)
    small = exchange(small)
    gain_grad = small[:, 0].reshape(-1) / value_gain
    mine = lax.axis_index(Z) * parts + lax.axis_index("sp_1")
    bias_grad = lax.dynamic_slice_in_dim(small, mine, 1, axis=0)[:, 1]
    up_grad, value_grad = epilogue(back, cot, up_slope, val_slope, act, inv, gain)
    return (up_grad[None], value_grad[None], grads[None].astype(F32), bias_grad, gain_grad)


def solution(mesh):
    torus = Mesh(mesh.devices.reshape(8, 4, 4, 2), ("sp_0", "sp_1", "dp_0", "dp_1"))
    in_specs = (
        P(DP, SP, None),
        P(DP, SP, None),
        P(DP, SP, None),
        P(SP, DP, None),
        P(SP, None),
        P(),
    )
    out_specs = (P(DP, SP, None), P(DP, SP, None), P(SP, DP, None), P(SP, DP), P())
    return jax.shard_map(
        shards, mesh=torus, in_specs=in_specs, out_specs=out_specs, check_vma=False
    )
```

```python
import functools
import math

import jax
import jax.numpy as jnp
from jax import lax
from jax.experimental import pallas as pl
from jax.experimental.pallas import tpu as pltpu
from jax.sharding import Mesh
from jax.sharding import PartitionSpec as P

Z = "sp_0"
SP = ("sp_0", "sp_1")
DP = ("dp_0", "dp_1")
PLANE = ("dp_0", "dp_1", "sp_1")
Z_DP = ("sp_0", "dp_0", "dp_1")

norm_floor = 0.5
root_half = 1.0 / math.sqrt(2.0)
inv_root_tau = 1.0 / math.sqrt(2.0 * math.pi)
LANES = 128
F32 = jnp.float32
BF16 = jnp.bfloat16


def normal_cdf(x):
    return 0.5 * (1.0 + lax.erf(x * root_half))


HBM = pl.BlockSpec(memory_space=pltpu.HBM)
VMEM = pl.BlockSpec(memory_space=pltpu.VMEM)


def limit(mib):
    return pltpu.CompilerParams(vmem_limit_bytes=mib * 1024 * 1024)


def params(mib):
    return pltpu.CompilerParams(
        dimension_semantics=("arbitrary",), vmem_limit_bytes=mib * 1024 * 1024
    )


def prologue_kernel(
    groups, rows, cot_hbm, up_hbm, val_hbm, gain_ref, out_hbm, inv_ref, cot_ref, up_ref, val_ref, out_ref, act_ref, sems
):
    toks = cot_ref.shape[0]
    steps = toks // rows

    def loads(i):
        at = pl.ds(pl.multiple_of(i * rows, rows), rows)
        pairs = ((cot_hbm, cot_ref), (up_hbm, up_ref), (val_hbm, val_ref))
        return [
            pltpu.make_async_copy(src.at[at], dst.at[at], sems.at[k, i])
            for k, (src, dst) in enumerate(pairs)
        ]

    def store(i):
        at = pl.ds(pl.multiple_of(i * rows, rows), rows)
        return pltpu.make_async_copy(out_ref.at[:, :, at], out_hbm.at[:, :, at], sems.at[3, i])

    for i in range(AHEAD):
        for copy in loads(i):
            copy.start()

    def step(i, carry):
        for copy in loads(i):
            copy.wait()

        @pl.when(i + AHEAD < steps)
        def _():
            for copy in loads(i + AHEAD):
                copy.start()

        at = pl.ds(pl.multiple_of(i * rows, rows), rows)

        def first(g, squares):
            cols = pl.ds(pl.multiple_of(g * LANES, LANES), LANES)
            up = up_ref[at, cols].astype(F32)
            up_act = (up * normal_cdf(up)).astype(BF16).astype(F32)
            out_ref[g, 0, at] = (cot_ref[at, cols].astype(F32) * up_act).astype(BF16)
            val = val_ref[at, cols].astype(F32)
            act = val * normal_cdf(val)
            act_ref[:, cols] = act
            return squares + act * act

        squares = lax.fori_loop(0, groups, first, jnp.zeros((rows, LANES), F32), unroll=UNROLL)
        mean = jnp.sum(squares, axis=1, keepdims=True) * (1.0 / (groups * LANES))
        inv = lax.rsqrt(mean + norm_floor)
        inv_ref[at] = jnp.broadcast_to(inv, (rows, LANES))

        def second(g, carry):
            cols = pl.ds(pl.multiple_of(g * LANES, LANES), LANES)
            out_ref[g, 1, at] = (act_ref[:, cols] * inv * gain_ref[:, cols]).astype(BF16)
            return carry

        lax.fori_loop(0, groups, second, 0, unroll=4)
        store(i).start()
        return carry

    lax.fori_loop(0, steps, step, 0)
    for i in range(steps):
        store(i).wait()


UNROLL = 4
AHEAD = 4


def prologue(cot, up, val, gain, rows=64):
    toks, width = cot.shape
    groups = width // LANES
    whole = pltpu.VMEM((toks, width), BF16)
    return pl.pallas_call(
        functools.partial(prologue_kernel, groups, rows),
        in_specs=[HBM, HBM, HBM, VMEM],
        out_specs=[HBM, VMEM],
        out_shape=[
            jax.ShapeDtypeStruct((groups, 2, toks, LANES), BF16),
            jax.ShapeDtypeStruct((toks, LANES), F32),
        ],
        scratch_shapes=[
            whole,
            whole,
            whole,
            pltpu.VMEM((groups, 2, toks, LANES), BF16),
            pltpu.VMEM((rows, width), F32),
            pltpu.SemaphoreType.DMA((4, toks // rows)),
        ],
        compiler_params=limit(60),
        cost_estimate=pl.CostEstimate(
            flops=100 * toks * width, bytes_accessed=10 * toks * width, transcendentals=0
        ),
        name="prologue",
    )(cot, up, val, gain)


def slopes_kernel(up_ref, val_ref, up_slope_ref, val_slope_ref, act_ref):
    groups = up_ref.shape[1] // LANES

    def step(g, carry):
        at = pl.ds(pl.multiple_of(g * LANES, LANES), LANES)
        up = up_ref[:, at].astype(F32)
        up_slope = normal_cdf(up) + up * (jnp.exp(-0.5 * up * up) * inv_root_tau)
        up_slope_ref[:, at] = up_slope.astype(BF16)
        val = val_ref[:, at].astype(F32)
        phi = normal_cdf(val)
        act_ref[:, at] = (val * phi).astype(BF16)
        val_slope = phi + val * (jnp.exp(-0.5 * val * val) * inv_root_tau)
        val_slope_ref[:, at] = val_slope.astype(BF16)
        return carry

    lax.fori_loop(0, groups, step, 0, unroll=2)


def slopes(up, val, rows=64):
    toks, width = up.shape
    row = pl.BlockSpec((rows, width), lambda i: (i, 0))
    out = jax.ShapeDtypeStruct((toks, width), BF16)
    return pl.pallas_call(
        slopes_kernel,
        grid=(toks // rows,),
        in_specs=[row, row],
        out_specs=[row, row, row],
        out_shape=[out, out, out],
        compiler_params=params(60),
        cost_estimate=pl.CostEstimate(
            flops=100 * toks * width, bytes_accessed=16 * toks * width, transcendentals=0
        ),
        name="slopes",
    )(up, val)


def slab_of(z_offset):
    z = (lax.axis_index(Z) + z_offset + 8) % 8
    return z ^ (lax.axis_index("dp_0") * 2 + lax.axis_index("dp_1"))


OFFSETS = (0, -1, -2, -3, 1, 2, 3, 4)
PAD = 8


def arrange_kernel(*refs):
    *pieces, w_ref, wt_ref = refs
    slab = pieces[0].shape[0]
    for d, piece in enumerate(pieces):
        at = pl.ds(pl.multiple_of(slab_of(OFFSETS[d]) * slab, slab), slab)
        rows = piece[...]
        w_ref[at] = rows
        wt_ref[:, at] = jnp.transpose(rows)


def arrange(pieces):
    _, block = pieces[0].shape
    return pl.pallas_call(
        arrange_kernel,
        in_specs=[VMEM] * len(pieces),
        out_specs=[VMEM] * 2,
        out_shape=[
            jax.ShapeDtypeStruct((block, block), BF16),
            jax.ShapeDtypeStruct((block, block), BF16),
        ],
        compiler_params=limit(8),
        cost_estimate=pl.CostEstimate(
            flops=4 * block * block, bytes_accessed=6 * block * block, transcendentals=0
        ),
        name="arrange",
    )(*pieces)


def mix_kernel(
    seqs, parts, per, recv_hbm, w_hbm, wt_hbm, bias_row_ref, out_hbm, sums_ref,
    recv_ref, out_ref, w_ref, wt_ref, bias_ref, sems, fixed_sems
):
    toks = recv_ref.shape[2]
    block = parts * toks
    steps = seqs // per

    def load(j):
        at = pl.ds(j * (per * parts), per * parts)
        return pltpu.make_async_copy(recv_hbm.at[at], recv_ref.at[at], sems.at[0, j])

    def store(j):
        at = pl.ds(j * per, per)
        return pltpu.make_async_copy(out_ref.at[at], out_hbm.at[at], sems.at[1, j])

    def side_by_side(j, which):
        return jnp.concatenate(
            [
                recv_ref[pl.ds((j * per + b) * parts, parts), which].reshape(block, LANES)
                for b in range(per)
            ],
            axis=1,
        )

    fixed = [
        pltpu.make_async_copy(src, dst, fixed_sems.at[k])
        for k, (src, dst) in enumerate(((wt_hbm, wt_ref), (w_hbm, w_ref)))
    ]
    fixed[0].start()
    load(0).start()
    fixed[1].start()
    for j in range(1, steps):
        load(j).start()
    bias_ref[...] = jnp.transpose(jnp.broadcast_to(bias_row_ref[...], (LANES, block)))
    fixed[0].wait()

    def step(j, total):
        load(j).wait()
        gate = side_by_side(j, 0)
        back = jnp.dot(wt_ref[...], gate, preferred_element_type=F32).astype(BF16)
        value = side_by_side(j, 1)
        for b in range(per):
            cols = slice(b * LANES, (b + 1) * LANES)
            out_ref[j * per + b, :, 1] = back[:, cols].reshape(parts, toks, LANES)
            terms = back[:, cols].astype(F32) * value[:, cols].astype(F32)
            total += jnp.sum(terms.reshape(block // 8, 8, LANES), axis=0)

        @pl.when(j == 0)
        def _():
            fixed[1].wait()

        mixed = jnp.dot(w_ref[...], value, preferred_element_type=F32)
        for b in range(per):
            cols = slice(b * LANES, (b + 1) * LANES)
            part = (mixed[:, cols] + bias_ref[...]).astype(BF16)
            out_ref[j * per + b, :, 0] = part.reshape(parts, toks, LANES)
        store(j).start()
        return total

    total = lax.fori_loop(0, steps, step, jnp.zeros((8, LANES), F32))
    sums_ref[...] = jnp.sum(total, axis=0, keepdims=True)
    for j in range(steps):
        store(j).wait()


PER = 4


def mix(recv, w, wt, bias, seqs, parts):
    toks = recv.shape[2]
    block = parts * toks
    whole = (seqs, parts, 2, toks, LANES)
    out, sums = pl.pallas_call(
        functools.partial(mix_kernel, seqs, parts, PER),
        in_specs=[HBM] * 3 + [VMEM],
        out_specs=[HBM, VMEM],
        out_shape=[jax.ShapeDtypeStruct(whole, BF16), jax.ShapeDtypeStruct((1, LANES), F32)],
        scratch_shapes=[
            pltpu.VMEM(recv.shape, BF16),
            pltpu.VMEM(whole, BF16),
            pltpu.VMEM((block, block), BF16),
            pltpu.VMEM((block, block), BF16),
            pltpu.VMEM((block, LANES), F32),
            pltpu.SemaphoreType.DMA((2, seqs // PER)),
            pltpu.SemaphoreType.DMA((2,)),
        ],
        compiler_params=limit(60),
        cost_estimate=pl.CostEstimate(
            flops=4 * block * block * seqs * LANES, bytes_accessed=10 * block * block, transcendentals=0
        ),
        name="mix",
    )(recv, w, wt, bias)
    return out.reshape(recv.shape), sums


def split(x):
    high = x.astype(BF16)
    middle = (x - high.astype(F32)).astype(BF16)
    low = (x - high.astype(F32) - middle.astype(F32)).astype(BF16)
    return high, middle, low


def pack_sums(sums):
    bias = split(sums[:, LANES:])
    wide = jnp.concatenate([sums[:, :LANES], jnp.zeros_like(sums[:, 2 * LANES :])], axis=1)
    gain = split(wide)
    zeros = jnp.zeros_like(bias[0])
    return jnp.concatenate([*bias, *gain, zeros, zeros], axis=0)


def unpack_sums(rows):
    rows = rows.astype(F32)
    bias = rows[0:1] + rows[1:2] + rows[2:3]
    gain = rows[3:4] + rows[4:5] + rows[5:6]
    return jnp.concatenate([gain[:, :LANES], bias], axis=1)


def grads_kernel(seqs, parts, recv_ref, sums_ref, *refs):
    outs = refs[:seqs]
    gate_ref, value_ref, grad_ref, rows_ref, sems = refs[seqs:]
    toks = recv_ref.shape[2]
    block = parts * toks
    slab = block // seqs
    for b in range(seqs):
        cols = slice(b * LANES, (b + 1) * LANES)
        pieces = slice(b * parts, (b + 1) * parts)
        pltpu.make_async_copy(recv_ref.at[pieces, 0], gate_ref.at[:, :, cols], sems.at[0, 0]).start()
        pltpu.make_async_copy(recv_ref.at[pieces, 1], value_ref.at[:, :, cols], sems.at[1, 0]).start()
    pltpu.make_async_copy(gate_ref, gate_ref, sems.at[0, 0]).wait()
    bias_sums = []
    for y in range(parts):
        gate = gate_ref[y].astype(F32)
        gate = sum(gate[:, b * LANES : (b + 1) * LANES] for b in range(seqs))
        bias_sums.append(jnp.sum(jnp.transpose(gate), axis=0, keepdims=True))
    rows_ref[...] = pack_sums(jnp.concatenate([sums_ref[...], *bias_sums], axis=1))
    for d in range(seqs):
        pltpu.make_async_copy(rows_ref, outs[d].at[slab:], sems.at[3, d]).start()
    pltpu.make_async_copy(value_ref, value_ref, sems.at[1, 0]).wait()

    def step(y, carry):
        grad = lax.dot_general(
            gate_ref[...].reshape(block, seqs * LANES),
            value_ref[y],
            (((1,), (1,)), ((), ())),
            preferred_element_type=F32,
        )
        grad_ref[y] = grad.astype(BF16)
        at = pl.ds(pl.multiple_of(y * toks, toks), toks)
        for d in range(seqs):
            rows = pl.ds(pl.multiple_of(slab_of(-OFFSETS[d]) * slab, slab), slab)
            pltpu.make_async_copy(grad_ref.at[y, rows], outs[d].at[:slab, at], sems.at[2, 0]).start()
        return carry

    lax.fori_loop(0, parts, step, 0)
    pltpu.make_async_copy(grad_ref, grad_ref, sems.at[2, 0]).wait()
    for d in range(seqs):
        pltpu.make_async_copy(rows_ref, outs[d].at[slab:], sems.at[3, d]).wait()


def weight_grads(recv, sums, seqs, parts):
    toks = recv.shape[2]
    block = parts * toks
    flat = pltpu.VMEM((parts, toks, seqs * LANES), BF16)
    return pl.pallas_call(
        functools.partial(grads_kernel, seqs, parts),
        in_specs=[HBM, VMEM],
        out_specs=[HBM] * seqs,
        out_shape=[jax.ShapeDtypeStruct((block // seqs + PAD, block), BF16)] * seqs,
        scratch_shapes=[
            flat,
            flat,
            pltpu.VMEM((parts, block, toks), BF16),
            pltpu.VMEM((PAD, block), BF16),
            pltpu.SemaphoreType.DMA((4, seqs)),
        ],
        compiler_params=limit(28),
        cost_estimate=pl.CostEstimate(
            flops=2 * block * block * seqs * LANES, bytes_accessed=6 * block * block, transcendentals=0
        ),
        name="weight_grads",
    )(recv, sums)


def hop_kernel(slab, *refs):
    n = len(refs) // 3
    for here, there, out in zip(refs[:n], refs[n : 2 * n], refs[2 * n :]):
        out[:slab] = (here[:slab].astype(F32) + there[:slab].astype(F32)).astype(BF16)
        out[slab:] = pack_sums(unpack_sums(here[slab:]) + unpack_sums(there[slab:]))


def hop(here, there):
    height, width = here[0].shape
    return pl.pallas_call(
        functools.partial(hop_kernel, height - PAD),
        in_specs=[VMEM] * (2 * len(here)),
        out_specs=[VMEM] * len(here),
        out_shape=[jax.ShapeDtypeStruct((height, width), BF16)] * len(here),
        compiler_params=limit(8),
        cost_estimate=pl.CostEstimate(
            flops=2 * height * width, bytes_accessed=12 * height * width, transcendentals=0
        ),
        name="hop",
    )(*here, *there)


def last_kernel(slab, *refs):
    *ins, grad_ref = refs
    grad_ref[...] = sum(r[:slab].astype(F32) for r in ins).astype(BF16)


def last(pieces):
    height, width = pieces[0].shape
    return pl.pallas_call(
        functools.partial(last_kernel, height - PAD),
        in_specs=[VMEM] * 3,
        out_specs=VMEM,
        out_shape=jax.ShapeDtypeStruct((height - PAD, width), BF16),
        compiler_params=limit(8),
        cost_estimate=pl.CostEstimate(
            flops=4 * height * width, bytes_accessed=8 * height * width, transcendentals=0
        ),
        name="last",
    )(*pieces)


def pack_kernel(slab, seqs, parts, *refs):
    *ins, gain_ref, small_ref = refs
    sums = sum(unpack_sums(r[slab:]) for r in ins)
    group = (lax.axis_index("dp_0") * 2 + lax.axis_index("dp_1")) * parts + lax.axis_index("sp_1")
    gain = gain_ref[:, pl.ds(pl.multiple_of(group * LANES, LANES), LANES)]
    gain_sum = sums[:, :LANES] / gain
    small_ref[...] = jnp.zeros_like(small_ref)
    for a in range(seqs):
        at = slice((a + 1) * LANES, (a + 2) * LANES)
        for y in range(parts):
            small_ref[a * parts + y, :1] = gain_sum
            small_ref[a * parts + y, 1:2] = sums[:, at]


def pack(pieces, gain, seqs, parts):
    slab = pieces[0].shape[0] - PAD
    return pl.pallas_call(
        functools.partial(pack_kernel, slab, seqs, parts),
        in_specs=[VMEM] * 4,
        out_specs=VMEM,
        out_shape=jax.ShapeDtypeStruct((seqs * parts, 8, LANES), F32),
        compiler_params=limit(8),
        name="pack",
    )(*pieces, gain)


def epilogue_kernel(
    groups, rows, recv_hbm, cot_hbm, up_slope_hbm, val_slope_hbm, act_hbm, inv_ref, gain_ref, up_hbm, val_hbm,
    recv_ref, cot_ref, up_slope_ref, val_slope_ref, act_ref, up_ref, val_ref, sems
):
    toks = cot_ref.shape[0]
    steps = toks // rows

    def loads(i):
        at = pl.ds(pl.multiple_of(i * rows, rows), rows)
        pairs = (
            (cot_hbm, cot_ref),
            (up_slope_hbm, up_slope_ref),
            (val_slope_hbm, val_slope_ref),
            (act_hbm, act_ref),
        )
        return [pltpu.make_async_copy(recv_hbm.at[:, :, at], recv_ref.at[:, :, at], sems.at[0, i])] + [
            pltpu.make_async_copy(src.at[at], dst.at[at], sems.at[3 + k, i])
            for k, (src, dst) in enumerate(pairs)
        ]

    def stores(i):
        at = pl.ds(pl.multiple_of(i * rows, rows), rows)
        return [
            pltpu.make_async_copy(up_ref.at[at], up_hbm.at[at], sems.at[1, i]),
            pltpu.make_async_copy(val_ref.at[at], val_hbm.at[at], sems.at[2, i]),
        ]

    for i in range(AHEAD):
        for copy in loads(i):
            copy.start()

    def step(i, carry):
        for copy in loads(i):
            copy.wait()

        @pl.when(i + AHEAD < steps)
        def _():
            for copy in loads(i + AHEAD):
                copy.start()

        at = pl.ds(pl.multiple_of(i * rows, rows), rows)

        def first(g, dots):
            cols = pl.ds(pl.multiple_of(g * LANES, LANES), LANES)
            mid = (cot_ref[at, cols].astype(F32) * recv_ref[g, 0, at].astype(F32)).astype(BF16)
            up_ref[at, cols] = (mid.astype(F32) * up_slope_ref[at, cols].astype(F32)).astype(BF16)
            scaled = recv_ref[g, 1, at].astype(F32) * gain_ref[:, cols]
            return dots + scaled * act_ref[at, cols].astype(F32)

        dots = lax.fori_loop(0, groups, first, jnp.zeros((rows, LANES), F32), unroll=4)
        mean = jnp.sum(dots, axis=1, keepdims=True) * (1.0 / (groups * LANES))
        inv = inv_ref[at]
        pull = inv * inv * inv * mean

        def second(g, carry):
            cols = pl.ds(pl.multiple_of(g * LANES, LANES), LANES)
            scaled = recv_ref[g, 1, at].astype(F32) * gain_ref[:, cols]
            slope = inv * scaled - pull * act_ref[at, cols].astype(F32)
            val_ref[at, cols] = (slope * val_slope_ref[at, cols].astype(F32)).astype(BF16)
            return carry

        lax.fori_loop(0, groups, second, 0, unroll=4)
        for copy in stores(i):
            copy.start()
        return carry

    lax.fori_loop(0, steps, step, 0)
    for i in range(steps):
        for copy in stores(i):
            copy.wait()


def epilogue(recv, cot, up_slope, val_slope, act, inv, gain, rows=64):
    toks, width = cot.shape
    groups = width // LANES
    out = jax.ShapeDtypeStruct((toks, width), BF16)
    whole = pltpu.VMEM((toks, width), BF16)
    return pl.pallas_call(
        functools.partial(epilogue_kernel, groups, rows),
        in_specs=[HBM] * 5 + [VMEM] * 2,
        out_specs=[HBM, HBM],
        out_shape=[out, out],
        scratch_shapes=[
            pltpu.VMEM(recv.shape, BF16),
            whole,
            whole,
            whole,
            whole,
            whole,
            whole,
            pltpu.SemaphoreType.DMA((7, toks // rows)),
        ],
        compiler_params=limit(EPI_MIB),
        cost_estimate=pl.CostEstimate(
            flops=20 * toks * width, bytes_accessed=22 * toks * width, transcendentals=0
        ),
        name="epilogue",
    )(recv, cot, up_slope, val_slope, act, inv, gain)


EPI_MIB = 60


def shards(cotangent, up_pre, value_pre, spatial_weight, spatial_bias, value_gain):
    planes = lax.axis_size(Z)
    seqs = lax.axis_size(DP)
    parts = lax.axis_size("sp_1")
    cot, up, val = cotangent[0], up_pre[0], value_pre[0]
    gain = value_gain[None]
    away = [(z * seqs + a, (z ^ a) * seqs + z) for z in range(planes) for a in range(seqs)]
    home = [(there, here) for here, there in away]

    def exchange(x):
        return lax.all_to_all(x, PLANE, split_axis=0, concat_axis=0, tiled=True)

    def shifted(x, by):
        return lax.ppermute(x, Z, [(z, (z + by) % planes) for z in range(planes)])

    weights = lax.ppermute(spatial_weight[0], Z_DP, away)
    bias = lax.ppermute(spatial_bias, Z_DP, away)
    sent, inv = prologue(cot, up, val, gain)
    recv = exchange(sent)
    before, after = [weights], [weights]
    for _ in range(3):
        before.append(shifted(before[-1], 1))
        after.append(shifted(after[-1], -1))
    after.append(shifted(after[-1], -1))
    pieces = before + after[1:]
    up_slope, val_slope, act = slopes(up, val)
    w, wt = arrange(pieces)
    back, sums = mix(recv, w, wt, bias, seqs, parts)
    back = exchange(back)
    own, p1, p2, p3, m1, m2, m3, m4 = weight_grads(recv, sums, seqs, parts)
    plus, minus = shifted(p3, 1), shifted(m4, -1)
    plus, minus = hop((p2, m3), (plus, minus))
    plus, minus = shifted(plus, 1), shifted(minus, -1)
    plus, minus = hop((p1, m2), (plus, minus))
    plus, minus = shifted(plus, 1), shifted(minus, -1)
    (minus,) = hop((m1,), (minus,))
    minus = shifted(minus, -1)
    grads = last((own, plus, minus))
    small = pack((own, plus, minus), gain, seqs, parts)
    grads, back = lax.optimization_barrier((grads, back))
    grads = lax.ppermute(grads, Z_DP, home)
    small = exchange(small)
    gain_grad = small[:, 0].reshape(-1)
    mine = lax.axis_index(Z) * parts + lax.axis_index("sp_1")
    bias_grad = lax.dynamic_slice_in_dim(small, mine, 1, axis=0)[:, 1]
    up_grad, value_grad = epilogue(back, cot, up_slope, val_slope, act, inv, gain)
    return (up_grad[None], value_grad[None], grads[None].astype(F32), bias_grad, gain_grad)


def solution(mesh):
    torus = Mesh(mesh.devices.reshape(8, 4, 4, 2), ("sp_0", "sp_1", "dp_0", "dp_1"))
    in_specs = (
        P(DP, SP, None),
        P(DP, SP, None),
        P(DP, SP, None),
        P(SP, DP, None),
        P(SP, None),
        P(),
    )
    out_specs = (P(DP, SP, None), P(DP, SP, None), P(SP, DP, None), P(SP, DP), P())
    return jax.shard_map(
        shards, mesh=torus, in_specs=in_specs, out_specs=out_specs, check_vma=False
    )
```

```python
import functools
import math

import jax
import jax.numpy as jnp
from jax import lax
from jax.experimental import pallas as pl
from jax.experimental.pallas import tpu as pltpu
from jax.sharding import Mesh
from jax.sharding import PartitionSpec as P

Z = "sp_0"
SP = ("sp_0", "sp_1")
DP = ("dp_0", "dp_1")
PLANE = ("dp_1", "dp_0", "sp_1")
Z_DP = ("sp_0", "dp_0", "dp_1")

norm_floor = 0.5
root_half = 1.0 / math.sqrt(2.0)
inv_root_tau = 1.0 / math.sqrt(2.0 * math.pi)
LANES = 128
F32 = jnp.float32
BF16 = jnp.bfloat16


def normal_cdf(x):
    return 0.5 * (1.0 + lax.erf(x * root_half))


HBM = pl.BlockSpec(memory_space=pltpu.HBM)
VMEM = pl.BlockSpec(memory_space=pltpu.VMEM)


def limit(mib):
    return pltpu.CompilerParams(vmem_limit_bytes=mib * 1024 * 1024)


def params(mib):
    return pltpu.CompilerParams(
        dimension_semantics=("arbitrary",), vmem_limit_bytes=mib * 1024 * 1024
    )


def prologue_kernel(
    groups, rows, cot_hbm, up_hbm, val_hbm, gain_ref, out_hbm, inv_ref, cot_ref, up_ref, val_ref, out_ref, act_ref, sems
):
    toks = cot_ref.shape[0]
    steps = toks // rows

    def loads(i):
        at = pl.ds(pl.multiple_of(i * rows, rows), rows)
        pairs = ((cot_hbm, cot_ref), (up_hbm, up_ref), (val_hbm, val_ref))
        return [
            pltpu.make_async_copy(src.at[at], dst.at[at], sems.at[k, i])
            for k, (src, dst) in enumerate(pairs)
        ]

    def store(i):
        at = pl.ds(pl.multiple_of(i * rows, rows), rows)
        return pltpu.make_async_copy(out_ref.at[:, :, at], out_hbm.at[:, :, at], sems.at[3, i])

    for i in range(AHEAD):
        for copy in loads(i):
            copy.start()

    def step(i, carry):
        for copy in loads(i):
            copy.wait()

        @pl.when(i + AHEAD < steps)
        def _():
            for copy in loads(i + AHEAD):
                copy.start()

        at = pl.ds(pl.multiple_of(i * rows, rows), rows)

        def first(g, squares):
            cols = pl.ds(pl.multiple_of(g * LANES, LANES), LANES)
            up = up_ref[at, cols].astype(F32)
            up_act = (up * normal_cdf(up)).astype(BF16).astype(F32)
            out_ref[g, 0, at] = (cot_ref[at, cols].astype(F32) * up_act).astype(BF16)
            val = val_ref[at, cols].astype(F32)
            act = val * normal_cdf(val)
            act_ref[:, cols] = act
            return squares + act * act

        squares = lax.fori_loop(0, groups, first, jnp.zeros((rows, LANES), F32), unroll=UNROLL)
        mean = jnp.sum(squares, axis=1, keepdims=True) * (1.0 / (groups * LANES))
        inv = lax.rsqrt(mean + norm_floor)
        inv_ref[at] = jnp.broadcast_to(inv, (rows, LANES))

        def second(g, carry):
            cols = pl.ds(pl.multiple_of(g * LANES, LANES), LANES)
            out_ref[g, 1, at] = (act_ref[:, cols] * inv * gain_ref[:, cols]).astype(BF16)
            return carry

        lax.fori_loop(0, groups, second, 0, unroll=4)
        store(i).start()
        return carry

    lax.fori_loop(0, steps, step, 0)
    for i in range(steps):
        store(i).wait()


UNROLL = 4
AHEAD = 4


def prologue(cot, up, val, gain, rows=64):
    toks, width = cot.shape
    groups = width // LANES
    whole = pltpu.VMEM((toks, width), BF16)
    return pl.pallas_call(
        functools.partial(prologue_kernel, groups, rows),
        in_specs=[HBM, HBM, HBM, VMEM],
        out_specs=[HBM, VMEM],
        out_shape=[
            jax.ShapeDtypeStruct((groups, 2, toks, LANES), BF16),
            jax.ShapeDtypeStruct((toks, LANES), F32),
        ],
        scratch_shapes=[
            whole,
            whole,
            whole,
            pltpu.VMEM((groups, 2, toks, LANES), BF16),
            pltpu.VMEM((rows, width), F32),
            pltpu.SemaphoreType.DMA((4, toks // rows)),
        ],
        compiler_params=limit(60),
        cost_estimate=pl.CostEstimate(
            flops=100 * toks * width, bytes_accessed=10 * toks * width, transcendentals=0
        ),
        name="prologue",
    )(cot, up, val, gain)


def slopes_kernel(up_ref, val_ref, up_slope_ref, val_slope_ref, act_ref):
    groups = up_ref.shape[1] // LANES

    def step(g, carry):
        at = pl.ds(pl.multiple_of(g * LANES, LANES), LANES)
        up = up_ref[:, at].astype(F32)
        up_slope = normal_cdf(up) + up * (jnp.exp(-0.5 * up * up) * inv_root_tau)
        up_slope_ref[:, at] = up_slope.astype(BF16)
        val = val_ref[:, at].astype(F32)
        phi = normal_cdf(val)
        act_ref[:, at] = (val * phi).astype(BF16)
        val_slope = phi + val * (jnp.exp(-0.5 * val * val) * inv_root_tau)
        val_slope_ref[:, at] = val_slope.astype(BF16)
        return carry

    lax.fori_loop(0, groups, step, 0, unroll=2)


def slopes(up, val, rows=64):
    toks, width = up.shape
    row = pl.BlockSpec((rows, width), lambda i: (i, 0))
    out = jax.ShapeDtypeStruct((toks, width), BF16)
    return pl.pallas_call(
        slopes_kernel,
        grid=(toks // rows,),
        in_specs=[row, row],
        out_specs=[row, row, row],
        out_shape=[out, out, out],
        compiler_params=params(60),
        cost_estimate=pl.CostEstimate(
            flops=100 * toks * width, bytes_accessed=16 * toks * width, transcendentals=0
        ),
        name="slopes",
    )(up, val)


def column():
    return lax.axis_index("dp_1") * 4 + lax.axis_index("dp_0")


def place(column):
    return column % 4 * 2 + column // 4


def slab_of(z_offset):
    return ((lax.axis_index(Z) + z_offset + 8) % 8) ^ column()


OFFSETS = (0, -1, -2, -3, 1, 2, 3, 4)
PAD = 8


def arrange_kernel(*refs):
    *pieces, w_ref, wt_ref = refs
    slab = pieces[0].shape[0]
    for d, piece in enumerate(pieces):
        at = pl.ds(pl.multiple_of(slab_of(OFFSETS[d]) * slab, slab), slab)
        rows = piece[...]
        w_ref[at] = rows
        wt_ref[:, at] = jnp.transpose(rows)


def arrange(pieces):
    _, block = pieces[0].shape
    return pl.pallas_call(
        arrange_kernel,
        in_specs=[VMEM] * len(pieces),
        out_specs=[VMEM] * 2,
        out_shape=[
            jax.ShapeDtypeStruct((block, block), BF16),
            jax.ShapeDtypeStruct((block, block), BF16),
        ],
        compiler_params=limit(8),
        cost_estimate=pl.CostEstimate(
            flops=4 * block * block, bytes_accessed=6 * block * block, transcendentals=0
        ),
        name="arrange",
    )(*pieces)


def mix_kernel(
    seqs, parts, per, recv_hbm, w_hbm, wt_hbm, bias_row_ref, out_hbm, sums_ref,
    recv_ref, out_ref, w_ref, wt_ref, bias_ref, sems, fixed_sems
):
    toks = recv_ref.shape[2]
    block = parts * toks
    steps = seqs // per

    def load(j):
        at = pl.ds(j * (per * parts), per * parts)
        return pltpu.make_async_copy(recv_hbm.at[at], recv_ref.at[at], sems.at[0, j])

    def store(j):
        at = pl.ds(j * per, per)
        return pltpu.make_async_copy(out_ref.at[at], out_hbm.at[at], sems.at[1, j])

    def side_by_side(j, which):
        return jnp.concatenate(
            [
                recv_ref[pl.ds((j * per + b) * parts, parts), which].reshape(block, LANES)
                for b in range(per)
            ],
            axis=1,
        )

    fixed = [
        pltpu.make_async_copy(src, dst, fixed_sems.at[k])
        for k, (src, dst) in enumerate(((wt_hbm, wt_ref), (w_hbm, w_ref)))
    ]
    fixed[0].start()
    load(0).start()
    fixed[1].start()
    for j in range(1, steps):
        load(j).start()
    bias_ref[...] = jnp.transpose(jnp.broadcast_to(bias_row_ref[...], (LANES, block)))
    fixed[0].wait()

    def step(j, total):
        load(j).wait()
        gate = side_by_side(j, 0)
        back = jnp.dot(wt_ref[...], gate, preferred_element_type=F32).astype(BF16)
        value = side_by_side(j, 1)
        for b in range(per):
            cols = slice(b * LANES, (b + 1) * LANES)
            out_ref[j * per + b, :, 1] = back[:, cols].reshape(parts, toks, LANES)
            terms = back[:, cols].astype(F32) * value[:, cols].astype(F32)
            total += jnp.sum(terms.reshape(block // 8, 8, LANES), axis=0)

        @pl.when(j == 0)
        def _():
            fixed[1].wait()

        mixed = jnp.dot(w_ref[...], value, preferred_element_type=F32)
        for b in range(per):
            cols = slice(b * LANES, (b + 1) * LANES)
            part = (mixed[:, cols] + bias_ref[...]).astype(BF16)
            out_ref[j * per + b, :, 0] = part.reshape(parts, toks, LANES)
        store(j).start()
        return total

    total = lax.fori_loop(0, steps, step, jnp.zeros((8, LANES), F32))
    sums_ref[...] = jnp.sum(total, axis=0, keepdims=True)
    for j in range(steps):
        store(j).wait()


PER = 4


def mix(recv, w, wt, bias, seqs, parts):
    toks = recv.shape[2]
    block = parts * toks
    whole = (seqs, parts, 2, toks, LANES)
    out, sums = pl.pallas_call(
        functools.partial(mix_kernel, seqs, parts, PER),
        in_specs=[HBM] * 3 + [VMEM],
        out_specs=[HBM, VMEM],
        out_shape=[jax.ShapeDtypeStruct(whole, BF16), jax.ShapeDtypeStruct((1, LANES), F32)],
        scratch_shapes=[
            pltpu.VMEM(recv.shape, BF16),
            pltpu.VMEM(whole, BF16),
            pltpu.VMEM((block, block), BF16),
            pltpu.VMEM((block, block), BF16),
            pltpu.VMEM((block, LANES), F32),
            pltpu.SemaphoreType.DMA((2, seqs // PER)),
            pltpu.SemaphoreType.DMA((2,)),
        ],
        compiler_params=limit(60),
        cost_estimate=pl.CostEstimate(
            flops=4 * block * block * seqs * LANES, bytes_accessed=10 * block * block, transcendentals=0
        ),
        name="mix",
    )(recv, w, wt, bias)
    return out.reshape(recv.shape), sums


def split(x):
    high = x.astype(BF16)
    middle = (x - high.astype(F32)).astype(BF16)
    low = (x - high.astype(F32) - middle.astype(F32)).astype(BF16)
    return high, middle, low


def pack_sums(sums):
    bias = split(sums[:, LANES:])
    wide = jnp.concatenate([sums[:, :LANES], jnp.zeros_like(sums[:, 2 * LANES :])], axis=1)
    gain = split(wide)
    zeros = jnp.zeros_like(bias[0])
    return jnp.concatenate([*bias, *gain, zeros, zeros], axis=0)


def unpack_sums(rows):
    rows = rows.astype(F32)
    bias = rows[0:1] + rows[1:2] + rows[2:3]
    gain = rows[3:4] + rows[4:5] + rows[5:6]
    return jnp.concatenate([gain[:, :LANES], bias], axis=1)


def grads_kernel(seqs, parts, recv_ref, sums_ref, *refs):
    outs = refs[:seqs]
    gate_ref, value_ref, grad_ref, rows_ref, sems = refs[seqs:]
    toks = recv_ref.shape[2]
    block = parts * toks
    slab = block // seqs
    for b in range(seqs):
        cols = slice(b * LANES, (b + 1) * LANES)
        pieces = slice(b * parts, (b + 1) * parts)
        pltpu.make_async_copy(recv_ref.at[pieces, 0], gate_ref.at[:, :, cols], sems.at[0, 0]).start()
        pltpu.make_async_copy(recv_ref.at[pieces, 1], value_ref.at[:, :, cols], sems.at[1, 0]).start()
    pltpu.make_async_copy(gate_ref, gate_ref, sems.at[0, 0]).wait()
    bias_sums = []
    for y in range(parts):
        gate = gate_ref[y].astype(F32)
        gate = sum(gate[:, b * LANES : (b + 1) * LANES] for b in range(seqs))
        bias_sums.append(jnp.sum(jnp.transpose(gate), axis=0, keepdims=True))
    rows_ref[...] = pack_sums(jnp.concatenate([sums_ref[...], *bias_sums], axis=1))
    for d in range(seqs):
        pltpu.make_async_copy(rows_ref, outs[d].at[slab:], sems.at[3, d]).start()
    pltpu.make_async_copy(value_ref, value_ref, sems.at[1, 0]).wait()

    def step(y, carry):
        grad = lax.dot_general(
            gate_ref[...].reshape(block, seqs * LANES),
            value_ref[y],
            (((1,), (1,)), ((), ())),
            preferred_element_type=F32,
        )
        grad_ref[y] = grad.astype(BF16)
        at = pl.ds(pl.multiple_of(y * toks, toks), toks)
        for d in range(seqs):
            rows = pl.ds(pl.multiple_of(slab_of(-OFFSETS[d]) * slab, slab), slab)
            pltpu.make_async_copy(grad_ref.at[y, rows], outs[d].at[:slab, at], sems.at[2, 0]).start()
        return carry

    lax.fori_loop(0, parts, step, 0)
    pltpu.make_async_copy(grad_ref, grad_ref, sems.at[2, 0]).wait()
    for d in range(seqs):
        pltpu.make_async_copy(rows_ref, outs[d].at[slab:], sems.at[3, d]).wait()


def weight_grads(recv, sums, seqs, parts):
    toks = recv.shape[2]
    block = parts * toks
    flat = pltpu.VMEM((parts, toks, seqs * LANES), BF16)
    return pl.pallas_call(
        functools.partial(grads_kernel, seqs, parts),
        in_specs=[HBM, VMEM],
        out_specs=[HBM] * seqs,
        out_shape=[jax.ShapeDtypeStruct((block // seqs + PAD, block), BF16)] * seqs,
        scratch_shapes=[
            flat,
            flat,
            pltpu.VMEM((parts, block, toks), BF16),
            pltpu.VMEM((PAD, block), BF16),
            pltpu.SemaphoreType.DMA((4, seqs)),
        ],
        compiler_params=limit(28),
        cost_estimate=pl.CostEstimate(
            flops=2 * block * block * seqs * LANES, bytes_accessed=6 * block * block, transcendentals=0
        ),
        name="weight_grads",
    )(recv, sums)


def hop_kernel(slab, *refs):
    n = len(refs) // 3
    for here, there, out in zip(refs[:n], refs[n : 2 * n], refs[2 * n :]):
        out[:slab] = (here[:slab].astype(F32) + there[:slab].astype(F32)).astype(BF16)
        out[slab:] = pack_sums(unpack_sums(here[slab:]) + unpack_sums(there[slab:]))


def hop(here, there):
    height, width = here[0].shape
    return pl.pallas_call(
        functools.partial(hop_kernel, height - PAD),
        in_specs=[VMEM] * (2 * len(here)),
        out_specs=[VMEM] * len(here),
        out_shape=[jax.ShapeDtypeStruct((height, width), BF16)] * len(here),
        compiler_params=limit(8),
        cost_estimate=pl.CostEstimate(
            flops=2 * height * width, bytes_accessed=12 * height * width, transcendentals=0
        ),
        name="hop",
    )(*here, *there)


def last_kernel(slab, *refs):
    *ins, grad_ref = refs
    grad_ref[...] = sum(r[:slab].astype(F32) for r in ins).astype(BF16)


def last(pieces):
    height, width = pieces[0].shape
    return pl.pallas_call(
        functools.partial(last_kernel, height - PAD),
        in_specs=[VMEM] * 3,
        out_specs=VMEM,
        out_shape=jax.ShapeDtypeStruct((height - PAD, width), BF16),
        compiler_params=limit(8),
        cost_estimate=pl.CostEstimate(
            flops=4 * height * width, bytes_accessed=8 * height * width, transcendentals=0
        ),
        name="last",
    )(*pieces)


def pack_kernel(slab, seqs, parts, *refs):
    *ins, gain_ref, small_ref = refs
    sums = sum(unpack_sums(r[slab:]) for r in ins)
    group = column() * parts + lax.axis_index("sp_1")
    gain = gain_ref[:, pl.ds(pl.multiple_of(group * LANES, LANES), LANES)]
    gain_sum = sums[:, :LANES] / gain
    small_ref[...] = jnp.zeros_like(small_ref)
    for a in range(seqs):
        at = slice((place(a) + 1) * LANES, (place(a) + 2) * LANES)
        for y in range(parts):
            small_ref[a * parts + y, :1] = gain_sum
            small_ref[a * parts + y, 1:2] = sums[:, at]


def pack(pieces, gain, seqs, parts):
    slab = pieces[0].shape[0] - PAD
    return pl.pallas_call(
        functools.partial(pack_kernel, slab, seqs, parts),
        in_specs=[VMEM] * 4,
        out_specs=VMEM,
        out_shape=jax.ShapeDtypeStruct((seqs * parts, 8, LANES), F32),
        compiler_params=limit(8),
        name="pack",
    )(*pieces, gain)


def epilogue_kernel(
    groups, rows, recv_hbm, cot_hbm, up_slope_hbm, val_slope_hbm, act_hbm, inv_ref, gain_ref, up_hbm, val_hbm,
    recv_ref, cot_ref, up_slope_ref, val_slope_ref, act_ref, up_ref, val_ref, sems
):
    toks = cot_ref.shape[0]
    steps = toks // rows

    def loads(i):
        at = pl.ds(pl.multiple_of(i * rows, rows), rows)
        pairs = (
            (cot_hbm, cot_ref),
            (up_slope_hbm, up_slope_ref),
            (val_slope_hbm, val_slope_ref),
            (act_hbm, act_ref),
        )
        return [pltpu.make_async_copy(recv_hbm.at[:, :, at], recv_ref.at[:, :, at], sems.at[0, i])] + [
            pltpu.make_async_copy(src.at[at], dst.at[at], sems.at[3 + k, i])
            for k, (src, dst) in enumerate(pairs)
        ]

    def stores(i):
        at = pl.ds(pl.multiple_of(i * rows, rows), rows)
        return [
            pltpu.make_async_copy(up_ref.at[at], up_hbm.at[at], sems.at[1, i]),
            pltpu.make_async_copy(val_ref.at[at], val_hbm.at[at], sems.at[2, i]),
        ]

    for i in range(AHEAD):
        for copy in loads(i):
            copy.start()

    def step(i, carry):
        for copy in loads(i):
            copy.wait()

        @pl.when(i + AHEAD < steps)
        def _():
            for copy in loads(i + AHEAD):
                copy.start()

        at = pl.ds(pl.multiple_of(i * rows, rows), rows)

        def first(g, dots):
            cols = pl.ds(pl.multiple_of(g * LANES, LANES), LANES)
            mid = (cot_ref[at, cols].astype(F32) * recv_ref[g, 0, at].astype(F32)).astype(BF16)
            up_ref[at, cols] = (mid.astype(F32) * up_slope_ref[at, cols].astype(F32)).astype(BF16)
            scaled = recv_ref[g, 1, at].astype(F32) * gain_ref[:, cols]
            return dots + scaled * act_ref[at, cols].astype(F32)

        dots = lax.fori_loop(0, groups, first, jnp.zeros((rows, LANES), F32), unroll=4)
        mean = jnp.sum(dots, axis=1, keepdims=True) * (1.0 / (groups * LANES))
        inv = inv_ref[at]
        pull = inv * inv * inv * mean

        def second(g, carry):
            cols = pl.ds(pl.multiple_of(g * LANES, LANES), LANES)
            scaled = recv_ref[g, 1, at].astype(F32) * gain_ref[:, cols]
            slope = inv * scaled - pull * act_ref[at, cols].astype(F32)
            val_ref[at, cols] = (slope * val_slope_ref[at, cols].astype(F32)).astype(BF16)
            return carry

        lax.fori_loop(0, groups, second, 0, unroll=4)
        for copy in stores(i):
            copy.start()
        return carry

    lax.fori_loop(0, steps, step, 0)
    for i in range(steps):
        for copy in stores(i):
            copy.wait()


def epilogue(recv, cot, up_slope, val_slope, act, inv, gain, rows=64):
    toks, width = cot.shape
    groups = width // LANES
    out = jax.ShapeDtypeStruct((toks, width), BF16)
    whole = pltpu.VMEM((toks, width), BF16)
    return pl.pallas_call(
        functools.partial(epilogue_kernel, groups, rows),
        in_specs=[HBM] * 5 + [VMEM] * 2,
        out_specs=[HBM, HBM],
        out_shape=[out, out],
        scratch_shapes=[
            pltpu.VMEM(recv.shape, BF16),
            whole,
            whole,
            whole,
            whole,
            whole,
            whole,
            pltpu.SemaphoreType.DMA((7, toks // rows)),
        ],
        compiler_params=limit(EPI_MIB),
        cost_estimate=pl.CostEstimate(
            flops=20 * toks * width, bytes_accessed=22 * toks * width, transcendentals=0
        ),
        name="epilogue",
    )(recv, cot, up_slope, val_slope, act, inv, gain)


EPI_MIB = 60


def shards(cotangent, up_pre, value_pre, spatial_weight, spatial_bias, value_gain):
    planes = lax.axis_size(Z)
    seqs = lax.axis_size(DP)
    parts = lax.axis_size("sp_1")
    cot, up, val = cotangent[0], up_pre[0], value_pre[0]
    gain = value_gain[None]
    away = [(z * seqs + a, (z ^ a) * seqs + place(z)) for z in range(planes) for a in range(seqs)]
    home = [(there, here) for here, there in away]

    def exchange(x):
        return lax.all_to_all(x, PLANE, split_axis=0, concat_axis=0, tiled=True)

    def shifted(x, by):
        return lax.ppermute(x, Z, [(z, (z + by) % planes) for z in range(planes)])

    bias = lax.ppermute(spatial_bias, Z_DP, away)
    sent, inv = prologue(cot, up, val, gain)
    weights, sent = lax.optimization_barrier((spatial_weight[0], sent))
    weights = lax.ppermute(weights, Z_DP, away)
    recv = exchange(sent)
    before, after = [weights], [weights]
    for _ in range(3):
        before.append(shifted(before[-1], 1))
        after.append(shifted(after[-1], -1))
    after.append(shifted(after[-1], -1))
    pieces = before + after[1:]
    up_slope, val_slope, act = slopes(up, val)
    w, wt = arrange(pieces)
    back, sums = mix(recv, w, wt, bias, seqs, parts)
    back = exchange(back)
    own, p1, p2, p3, m1, m2, m3, m4 = weight_grads(recv, sums, seqs, parts)
    plus, minus = shifted(p3, 1), shifted(m4, -1)
    plus, minus = hop((p2, m3), (plus, minus))
    plus, minus = shifted(plus, 1), shifted(minus, -1)
    plus, minus = hop((p1, m2), (plus, minus))
    plus, minus = shifted(plus, 1), shifted(minus, -1)
    (minus,) = hop((m1,), (minus,))
    minus = shifted(minus, -1)
    grads = last((own, plus, minus))
    small = pack((own, plus, minus), gain, seqs, parts)
    grads, back = lax.optimization_barrier((grads, back))
    grads = lax.ppermute(grads, Z_DP, home)
    small = exchange(small)
    gain_grad = small[:, 0].reshape(-1)
    mine = lax.axis_index(Z) * parts + lax.axis_index("sp_1")
    bias_grad = lax.dynamic_slice_in_dim(small, mine, 1, axis=0)[:, 1]
    up_grad, value_grad = epilogue(back, cot, up_slope, val_slope, act, inv, gain)
    return (up_grad[None], value_grad[None], grads[None].astype(F32), bias_grad, gain_grad)


def solution(mesh):
    torus = Mesh(mesh.devices.reshape(8, 4, 4, 2), ("sp_0", "sp_1", "dp_0", "dp_1"))
    in_specs = (
        P(DP, SP, None),
        P(DP, SP, None),
        P(DP, SP, None),
        P(SP, DP, None),
        P(SP, None),
        P(),
    )
    out_specs = (P(DP, SP, None), P(DP, SP, None), P(SP, DP, None), P(SP, DP), P())
    return jax.shard_map(
        shards, mesh=torus, in_specs=in_specs, out_specs=out_specs, check_vma=False
    )
```

```python
import functools
import math

import jax
import jax.numpy as jnp
from jax import lax
from jax.experimental import pallas as pl
from jax.experimental.pallas import tpu as pltpu
from jax.sharding import Mesh
from jax.sharding import PartitionSpec as P

Z = "sp_0"
SP = ("sp_0", "sp_1")
DP = ("dp_0", "dp_1")
PLANE = ("dp_0", "dp_1", "sp_1")
Z_DP = ("sp_0", "dp_0", "dp_1")

norm_floor = 0.5
root_half = 1.0 / math.sqrt(2.0)
inv_root_tau = 1.0 / math.sqrt(2.0 * math.pi)
LANES = 128
F32 = jnp.float32
BF16 = jnp.bfloat16


def normal_cdf(x):
    return 0.5 * (1.0 + lax.erf(x * root_half))


HBM = pl.BlockSpec(memory_space=pltpu.HBM)
VMEM = pl.BlockSpec(memory_space=pltpu.VMEM)


def limit(mib):
    return pltpu.CompilerParams(vmem_limit_bytes=mib * 1024 * 1024)


def params(mib):
    return pltpu.CompilerParams(
        dimension_semantics=("arbitrary",), vmem_limit_bytes=mib * 1024 * 1024
    )


def prologue_kernel(
    groups, rows, cot_hbm, up_hbm, val_hbm, gain_ref, out_hbm, inv_ref, cot_ref, up_ref, val_ref, out_ref, act_ref, sems
):
    toks = cot_ref.shape[0]
    steps = toks // rows

    def loads(i):
        at = pl.ds(pl.multiple_of(i * rows, rows), rows)
        pairs = ((cot_hbm, cot_ref), (up_hbm, up_ref), (val_hbm, val_ref))
        return [
            pltpu.make_async_copy(src.at[at], dst.at[at], sems.at[k, i])
            for k, (src, dst) in enumerate(pairs)
        ]

    def store(i):
        at = pl.ds(pl.multiple_of(i * rows, rows), rows)
        return pltpu.make_async_copy(out_ref.at[:, :, at], out_hbm.at[:, :, at], sems.at[3, i])

    for i in range(AHEAD):
        for copy in loads(i):
            copy.start()

    def step(i, carry):
        for copy in loads(i):
            copy.wait()

        @pl.when(i + AHEAD < steps)
        def _():
            for copy in loads(i + AHEAD):
                copy.start()

        at = pl.ds(pl.multiple_of(i * rows, rows), rows)

        def first(g, squares):
            cols = pl.ds(pl.multiple_of(g * LANES, LANES), LANES)
            up = up_ref[at, cols].astype(F32)
            up_act = (up * normal_cdf(up)).astype(BF16).astype(F32)
            out_ref[block_of(g), 0, at] = (cot_ref[at, cols].astype(F32) * up_act).astype(BF16)
            val = val_ref[at, cols].astype(F32)
            act = val * normal_cdf(val)
            act_ref[:, cols] = act
            return squares + act * act

        squares = lax.fori_loop(0, groups, first, jnp.zeros((rows, LANES), F32), unroll=UNROLL)
        mean = jnp.sum(squares, axis=1, keepdims=True) * (1.0 / (groups * LANES))
        inv = lax.rsqrt(mean + norm_floor)
        inv_ref[at] = jnp.broadcast_to(inv, (rows, LANES))

        def second(g, carry):
            cols = pl.ds(pl.multiple_of(g * LANES, LANES), LANES)
            out_ref[block_of(g), 1, at] = (act_ref[:, cols] * inv * gain_ref[:, cols]).astype(BF16)
            return carry

        lax.fori_loop(0, groups, second, 0, unroll=4)
        store(i).start()
        return carry

    lax.fori_loop(0, steps, step, 0)
    for i in range(steps):
        store(i).wait()


UNROLL = 4
AHEAD = 4


def prologue(cot, up, val, gain, rows=64):
    toks, width = cot.shape
    groups = width // LANES
    whole = pltpu.VMEM((toks, width), BF16)
    return pl.pallas_call(
        functools.partial(prologue_kernel, groups, rows),
        in_specs=[HBM, HBM, HBM, VMEM],
        out_specs=[HBM, VMEM],
        out_shape=[
            jax.ShapeDtypeStruct((groups, 2, toks, LANES), BF16),
            jax.ShapeDtypeStruct((toks, LANES), F32),
        ],
        scratch_shapes=[
            whole,
            whole,
            whole,
            pltpu.VMEM((groups, 2, toks, LANES), BF16),
            pltpu.VMEM((rows, width), F32),
            pltpu.SemaphoreType.DMA((4, toks // rows)),
        ],
        compiler_params=limit(60),
        cost_estimate=pl.CostEstimate(
            flops=100 * toks * width, bytes_accessed=10 * toks * width, transcendentals=0
        ),
        name="prologue",
    )(cot, up, val, gain)


def slopes_kernel(up_ref, val_ref, up_slope_ref, val_slope_ref, act_ref):
    groups = up_ref.shape[1] // LANES

    def step(g, carry):
        at = pl.ds(pl.multiple_of(g * LANES, LANES), LANES)
        up = up_ref[:, at].astype(F32)
        up_slope = normal_cdf(up) + up * (jnp.exp(-0.5 * up * up) * inv_root_tau)
        up_slope_ref[:, at] = up_slope.astype(BF16)
        val = val_ref[:, at].astype(F32)
        phi = normal_cdf(val)
        act_ref[:, at] = (val * phi).astype(BF16)
        val_slope = phi + val * (jnp.exp(-0.5 * val * val) * inv_root_tau)
        val_slope_ref[:, at] = val_slope.astype(BF16)
        return carry

    lax.fori_loop(0, groups, step, 0, unroll=2)


def slopes(up, val, rows=64):
    toks, width = up.shape
    row = pl.BlockSpec((rows, width), lambda i: (i, 0))
    out = jax.ShapeDtypeStruct((toks, width), BF16)
    return pl.pallas_call(
        slopes_kernel,
        grid=(toks // rows,),
        in_specs=[row, row],
        out_specs=[row, row, row],
        out_shape=[out, out, out],
        compiler_params=params(60),
        cost_estimate=pl.CostEstimate(
            flops=100 * toks * width, bytes_accessed=16 * toks * width, transcendentals=0
        ),
        name="slopes",
    )(up, val)


def column():
    return lax.axis_index("dp_1") * 4 + lax.axis_index("dp_0")


def place(column):
    return column % 4 * 2 + column // 4


def block_of(group):
    at = group >> 2
    return ((at & 3) * 2 + (at >> 2)) * 4 + (group & 3)


def slab_of(z_offset):
    return ((lax.axis_index(Z) + z_offset + 8) % 8) ^ column()


OFFSETS = (0, -1, -2, -3, 1, 2, 3, 4)
PAD = 8


def arrange_kernel(*refs):
    *pieces, w_ref, wt_ref = refs
    slab = pieces[0].shape[0]
    for d, piece in enumerate(pieces):
        at = pl.ds(pl.multiple_of(slab_of(OFFSETS[d]) * slab, slab), slab)
        rows = piece[...]
        w_ref[at] = rows
        wt_ref[:, at] = jnp.transpose(rows)


def arrange(pieces):
    _, block = pieces[0].shape
    return pl.pallas_call(
        arrange_kernel,
        in_specs=[VMEM] * len(pieces),
        out_specs=[VMEM] * 2,
        out_shape=[
            jax.ShapeDtypeStruct((block, block), BF16),
            jax.ShapeDtypeStruct((block, block), BF16),
        ],
        compiler_params=limit(8),
        cost_estimate=pl.CostEstimate(
            flops=4 * block * block, bytes_accessed=6 * block * block, transcendentals=0
        ),
        name="arrange",
    )(*pieces)


def mix_kernel(
    seqs, parts, per, recv_hbm, w_hbm, wt_hbm, bias_row_ref, out_hbm, sums_ref,
    recv_ref, out_ref, w_ref, wt_ref, bias_ref, sems, fixed_sems
):
    toks = recv_ref.shape[2]
    block = parts * toks
    steps = seqs // per

    def load(j):
        at = pl.ds(j * (per * parts), per * parts)
        return pltpu.make_async_copy(recv_hbm.at[at], recv_ref.at[at], sems.at[0, j])

    def store(j):
        at = pl.ds(j * per, per)
        return pltpu.make_async_copy(out_ref.at[at], out_hbm.at[at], sems.at[1, j])

    def side_by_side(j, which):
        return jnp.concatenate(
            [
                recv_ref[pl.ds((j * per + b) * parts, parts), which].reshape(block, LANES)
                for b in range(per)
            ],
            axis=1,
        )

    fixed = [
        pltpu.make_async_copy(src, dst, fixed_sems.at[k])
        for k, (src, dst) in enumerate(((wt_hbm, wt_ref), (w_hbm, w_ref)))
    ]
    fixed[0].start()
    load(0).start()
    fixed[1].start()
    for j in range(1, steps):
        load(j).start()
    bias_ref[...] = jnp.transpose(jnp.broadcast_to(bias_row_ref[...], (LANES, block)))
    fixed[0].wait()

    def step(j, total):
        load(j).wait()
        gate = side_by_side(j, 0)
        back = jnp.dot(wt_ref[...], gate, preferred_element_type=F32).astype(BF16)
        value = side_by_side(j, 1)
        for b in range(per):
            cols = slice(b * LANES, (b + 1) * LANES)
            out_ref[j * per + b, :, 1] = back[:, cols].reshape(parts, toks, LANES)
            terms = back[:, cols].astype(F32) * value[:, cols].astype(F32)
            total += jnp.sum(terms.reshape(block // 8, 8, LANES), axis=0)

        @pl.when(j == 0)
        def _():
            fixed[1].wait()

        mixed = jnp.dot(w_ref[...], value, preferred_element_type=F32)
        for b in range(per):
            cols = slice(b * LANES, (b + 1) * LANES)
            part = (mixed[:, cols] + bias_ref[...]).astype(BF16)
            out_ref[j * per + b, :, 0] = part.reshape(parts, toks, LANES)
        store(j).start()
        return total

    total = lax.fori_loop(0, steps, step, jnp.zeros((8, LANES), F32))
    sums_ref[...] = jnp.sum(total, axis=0, keepdims=True)
    for j in range(steps):
        store(j).wait()


PER = 4


def mix(recv, w, wt, bias, seqs, parts):
    toks = recv.shape[2]
    block = parts * toks
    whole = (seqs, parts, 2, toks, LANES)
    out, sums = pl.pallas_call(
        functools.partial(mix_kernel, seqs, parts, PER),
        in_specs=[HBM] * 3 + [VMEM],
        out_specs=[HBM, VMEM],
        out_shape=[jax.ShapeDtypeStruct(whole, BF16), jax.ShapeDtypeStruct((1, LANES), F32)],
        scratch_shapes=[
            pltpu.VMEM(recv.shape, BF16),
            pltpu.VMEM(whole, BF16),
            pltpu.VMEM((block, block), BF16),
            pltpu.VMEM((block, block), BF16),
            pltpu.VMEM((block, LANES), F32),
            pltpu.SemaphoreType.DMA((2, seqs // PER)),
            pltpu.SemaphoreType.DMA((2,)),
        ],
        compiler_params=limit(60),
        cost_estimate=pl.CostEstimate(
            flops=4 * block * block * seqs * LANES, bytes_accessed=10 * block * block, transcendentals=0
        ),
        name="mix",
    )(recv, w, wt, bias)
    return out.reshape(recv.shape), sums


def split(x):
    high = x.astype(BF16)
    middle = (x - high.astype(F32)).astype(BF16)
    low = (x - high.astype(F32) - middle.astype(F32)).astype(BF16)
    return high, middle, low


def pack_sums(sums):
    bias = split(sums[:, LANES:])
    wide = jnp.concatenate([sums[:, :LANES], jnp.zeros_like(sums[:, 2 * LANES :])], axis=1)
    gain = split(wide)
    zeros = jnp.zeros_like(bias[0])
    return jnp.concatenate([*bias, *gain, zeros, zeros], axis=0)


def unpack_sums(rows):
    rows = rows.astype(F32)
    bias = rows[0:1] + rows[1:2] + rows[2:3]
    gain = rows[3:4] + rows[4:5] + rows[5:6]
    return jnp.concatenate([gain[:, :LANES], bias], axis=1)


def grads_kernel(seqs, parts, recv_ref, sums_ref, *refs):
    outs = refs[:seqs]
    gate_ref, value_ref, grad_ref, rows_ref, sems = refs[seqs:]
    toks = recv_ref.shape[2]
    block = parts * toks
    slab = block // seqs
    for b in range(seqs):
        cols = slice(b * LANES, (b + 1) * LANES)
        pieces = slice(b * parts, (b + 1) * parts)
        pltpu.make_async_copy(recv_ref.at[pieces, 0], gate_ref.at[:, :, cols], sems.at[0, 0]).start()
        pltpu.make_async_copy(recv_ref.at[pieces, 1], value_ref.at[:, :, cols], sems.at[1, 0]).start()
    pltpu.make_async_copy(gate_ref, gate_ref, sems.at[0, 0]).wait()
    bias_sums = []
    for y in range(parts):
        gate = gate_ref[y].astype(F32)
        gate = sum(gate[:, b * LANES : (b + 1) * LANES] for b in range(seqs))
        bias_sums.append(jnp.sum(jnp.transpose(gate), axis=0, keepdims=True))
    rows_ref[...] = pack_sums(jnp.concatenate([sums_ref[...], *bias_sums], axis=1))
    for d in range(seqs):
        pltpu.make_async_copy(rows_ref, outs[d].at[slab:], sems.at[3, d]).start()
    pltpu.make_async_copy(value_ref, value_ref, sems.at[1, 0]).wait()

    def step(y, carry):
        grad = lax.dot_general(
            gate_ref[...].reshape(block, seqs * LANES),
            value_ref[y],
            (((1,), (1,)), ((), ())),
            preferred_element_type=F32,
        )
        grad_ref[y] = grad.astype(BF16)
        at = pl.ds(pl.multiple_of(y * toks, toks), toks)
        for d in range(seqs):
            rows = pl.ds(pl.multiple_of(slab_of(-OFFSETS[d]) * slab, slab), slab)
            pltpu.make_async_copy(grad_ref.at[y, rows], outs[d].at[:slab, at], sems.at[2, 0]).start()
        return carry

    lax.fori_loop(0, parts, step, 0)
    pltpu.make_async_copy(grad_ref, grad_ref, sems.at[2, 0]).wait()
    for d in range(seqs):
        pltpu.make_async_copy(rows_ref, outs[d].at[slab:], sems.at[3, d]).wait()


def weight_grads(recv, sums, seqs, parts):
    toks = recv.shape[2]
    block = parts * toks
    flat = pltpu.VMEM((parts, toks, seqs * LANES), BF16)
    return pl.pallas_call(
        functools.partial(grads_kernel, seqs, parts),
        in_specs=[HBM, VMEM],
        out_specs=[HBM] * seqs,
        out_shape=[jax.ShapeDtypeStruct((block // seqs + PAD, block), BF16)] * seqs,
        scratch_shapes=[
            flat,
            flat,
            pltpu.VMEM((parts, block, toks), BF16),
            pltpu.VMEM((PAD, block), BF16),
            pltpu.SemaphoreType.DMA((4, seqs)),
        ],
        compiler_params=limit(28),
        cost_estimate=pl.CostEstimate(
            flops=2 * block * block * seqs * LANES, bytes_accessed=6 * block * block, transcendentals=0
        ),
        name="weight_grads",
    )(recv, sums)


def hop_kernel(slab, *refs):
    n = len(refs) // 3
    for here, there, out in zip(refs[:n], refs[n : 2 * n], refs[2 * n :]):
        out[:slab] = (here[:slab].astype(F32) + there[:slab].astype(F32)).astype(BF16)
        out[slab:] = pack_sums(unpack_sums(here[slab:]) + unpack_sums(there[slab:]))


def hop(here, there):
    height, width = here[0].shape
    return pl.pallas_call(
        functools.partial(hop_kernel, height - PAD),
        in_specs=[VMEM] * (2 * len(here)),
        out_specs=[VMEM] * len(here),
        out_shape=[jax.ShapeDtypeStruct((height, width), BF16)] * len(here),
        compiler_params=limit(8),
        cost_estimate=pl.CostEstimate(
            flops=2 * height * width, bytes_accessed=12 * height * width, transcendentals=0
        ),
        name="hop",
    )(*here, *there)


def last_kernel(slab, *refs):
    *ins, grad_ref = refs
    grad_ref[...] = sum(r[:slab].astype(F32) for r in ins).astype(BF16)


def last(pieces):
    height, width = pieces[0].shape
    return pl.pallas_call(
        functools.partial(last_kernel, height - PAD),
        in_specs=[VMEM] * 3,
        out_specs=VMEM,
        out_shape=jax.ShapeDtypeStruct((height - PAD, width), BF16),
        compiler_params=limit(8),
        cost_estimate=pl.CostEstimate(
            flops=4 * height * width, bytes_accessed=8 * height * width, transcendentals=0
        ),
        name="last",
    )(*pieces)


def pack_kernel(slab, seqs, parts, *refs):
    *ins, gain_ref, small_ref = refs
    sums = sum(unpack_sums(r[slab:]) for r in ins)
    group = column() * parts + lax.axis_index("sp_1")
    gain = gain_ref[:, pl.ds(pl.multiple_of(group * LANES, LANES), LANES)]
    gain_sum = sums[:, :LANES] / gain
    small_ref[...] = jnp.zeros_like(small_ref)
    for a in range(seqs):
        at = slice((a + 1) * LANES, (a + 2) * LANES)
        for y in range(parts):
            small_ref[a * parts + y, :1] = gain_sum
            small_ref[a * parts + y, 1:2] = sums[:, at]


def pack(pieces, gain, seqs, parts):
    slab = pieces[0].shape[0] - PAD
    return pl.pallas_call(
        functools.partial(pack_kernel, slab, seqs, parts),
        in_specs=[VMEM] * 4,
        out_specs=VMEM,
        out_shape=jax.ShapeDtypeStruct((seqs * parts, 8, LANES), F32),
        compiler_params=limit(8),
        name="pack",
    )(*pieces, gain)


def unpack_kernel(parts, small_ref, gain_ref, bias_ref):
    for group in range(small_ref.shape[0]):
        gain_ref[group : group + 1] = small_ref[block_of(group), :1]
    mine = place(lax.axis_index(Z)) * parts + lax.axis_index("sp_1")
    bias_ref[...] = small_ref[mine, 1:2]


def unpack(small, parts):
    count = small.shape[0]
    gain, bias = pl.pallas_call(
        functools.partial(unpack_kernel, parts),
        in_specs=[VMEM],
        out_specs=[VMEM] * 2,
        out_shape=[
            jax.ShapeDtypeStruct((count, LANES), F32),
            jax.ShapeDtypeStruct((1, LANES), F32),
        ],
        compiler_params=limit(8),
        name="unpack",
    )(small)
    return gain.reshape(-1), bias


def epilogue_kernel(
    groups, rows, recv_hbm, cot_hbm, up_slope_hbm, val_slope_hbm, act_hbm, inv_ref, gain_ref, up_hbm, val_hbm,
    recv_ref, cot_ref, up_slope_ref, val_slope_ref, act_ref, up_ref, val_ref, sems
):
    toks = cot_ref.shape[0]
    steps = toks // rows

    def loads(i):
        at = pl.ds(pl.multiple_of(i * rows, rows), rows)
        pairs = (
            (cot_hbm, cot_ref),
            (up_slope_hbm, up_slope_ref),
            (val_slope_hbm, val_slope_ref),
            (act_hbm, act_ref),
        )
        return [pltpu.make_async_copy(recv_hbm.at[:, :, at], recv_ref.at[:, :, at], sems.at[0, i])] + [
            pltpu.make_async_copy(src.at[at], dst.at[at], sems.at[3 + k, i])
            for k, (src, dst) in enumerate(pairs)
        ]

    def stores(i):
        at = pl.ds(pl.multiple_of(i * rows, rows), rows)
        return [
            pltpu.make_async_copy(up_ref.at[at], up_hbm.at[at], sems.at[1, i]),
            pltpu.make_async_copy(val_ref.at[at], val_hbm.at[at], sems.at[2, i]),
        ]

    for i in range(AHEAD):
        for copy in loads(i):
            copy.start()

    def step(i, carry):
        for copy in loads(i):
            copy.wait()

        @pl.when(i + AHEAD < steps)
        def _():
            for copy in loads(i + AHEAD):
                copy.start()

        at = pl.ds(pl.multiple_of(i * rows, rows), rows)

        def first(g, dots):
            cols = pl.ds(pl.multiple_of(g * LANES, LANES), LANES)
            mid = (cot_ref[at, cols].astype(F32) * recv_ref[block_of(g), 0, at].astype(F32)).astype(BF16)
            up_ref[at, cols] = (mid.astype(F32) * up_slope_ref[at, cols].astype(F32)).astype(BF16)
            scaled = recv_ref[block_of(g), 1, at].astype(F32) * gain_ref[:, cols]
            return dots + scaled * act_ref[at, cols].astype(F32)

        dots = lax.fori_loop(0, groups, first, jnp.zeros((rows, LANES), F32), unroll=4)
        mean = jnp.sum(dots, axis=1, keepdims=True) * (1.0 / (groups * LANES))
        inv = inv_ref[at]
        pull = inv * inv * inv * mean

        def second(g, carry):
            cols = pl.ds(pl.multiple_of(g * LANES, LANES), LANES)
            scaled = recv_ref[block_of(g), 1, at].astype(F32) * gain_ref[:, cols]
            slope = inv * scaled - pull * act_ref[at, cols].astype(F32)
            val_ref[at, cols] = (slope * val_slope_ref[at, cols].astype(F32)).astype(BF16)
            return carry

        lax.fori_loop(0, groups, second, 0, unroll=4)
        for copy in stores(i):
            copy.start()
        return carry

    lax.fori_loop(0, steps, step, 0)
    for i in range(steps):
        for copy in stores(i):
            copy.wait()


def epilogue(recv, cot, up_slope, val_slope, act, inv, gain, rows=64):
    toks, width = cot.shape
    groups = width // LANES
    out = jax.ShapeDtypeStruct((toks, width), BF16)
    whole = pltpu.VMEM((toks, width), BF16)
    return pl.pallas_call(
        functools.partial(epilogue_kernel, groups, rows),
        in_specs=[HBM] * 5 + [VMEM] * 2,
        out_specs=[HBM, HBM],
        out_shape=[out, out],
        scratch_shapes=[
            pltpu.VMEM(recv.shape, BF16),
            whole,
            whole,
            whole,
            whole,
            whole,
            whole,
            pltpu.SemaphoreType.DMA((7, toks // rows)),
        ],
        compiler_params=limit(EPI_MIB),
        cost_estimate=pl.CostEstimate(
            flops=20 * toks * width, bytes_accessed=22 * toks * width, transcendentals=0
        ),
        name="epilogue",
    )(recv, cot, up_slope, val_slope, act, inv, gain)


EPI_MIB = 60


def shards(cotangent, up_pre, value_pre, spatial_weight, spatial_bias, value_gain):
    planes = lax.axis_size(Z)
    seqs = lax.axis_size(DP)
    parts = lax.axis_size("sp_1")
    cot, up, val = cotangent[0], up_pre[0], value_pre[0]
    gain = value_gain[None]
    away = [(z * seqs + a, (z ^ a) * seqs + place(z)) for z in range(planes) for a in range(seqs)]
    home = [(there, here) for here, there in away]

    def exchange(x):
        return lax.all_to_all(x, PLANE, split_axis=0, concat_axis=0, tiled=True)

    def shifted(x, by):
        return lax.ppermute(x, Z, [(z, (z + by) % planes) for z in range(planes)])

    bias = lax.ppermute(spatial_bias, Z_DP, away)
    weights = lax.ppermute(spatial_weight[0], Z_DP, away)
    sent, inv = prologue(cot, up, val, gain)
    recv = exchange(sent)
    before, after = [weights], [weights]
    for _ in range(3):
        before.append(shifted(before[-1], 1))
        after.append(shifted(after[-1], -1))
    after.append(shifted(after[-1], -1))
    pieces = before + after[1:]
    up_slope, val_slope, act = slopes(up, val)
    w, wt = arrange(pieces)
    back, sums = mix(recv, w, wt, bias, seqs, parts)
    back = exchange(back)
    own, p1, p2, p3, m1, m2, m3, m4 = weight_grads(recv, sums, seqs, parts)
    plus, minus = shifted(p3, 1), shifted(m4, -1)
    plus, minus = hop((p2, m3), (plus, minus))
    plus, minus = shifted(plus, 1), shifted(minus, -1)
    plus, minus = hop((p1, m2), (plus, minus))
    plus, minus = shifted(plus, 1), shifted(minus, -1)
    (minus,) = hop((m1,), (minus,))
    minus = shifted(minus, -1)
    grads = last((own, plus, minus))
    small = pack((own, plus, minus), gain, seqs, parts)
    grads, back = lax.optimization_barrier((grads, back))
    grads = lax.ppermute(grads, Z_DP, home)
    small = exchange(small)
    gain_grad, bias_grad = unpack(small, parts)
    up_grad, value_grad = epilogue(back, cot, up_slope, val_slope, act, inv, gain)
    return (up_grad[None], value_grad[None], grads[None].astype(F32), bias_grad, gain_grad)


def solution(mesh):
    torus = Mesh(mesh.devices.reshape(8, 4, 4, 2), ("sp_0", "sp_1", "dp_0", "dp_1"))
    in_specs = (
        P(DP, SP, None),
        P(DP, SP, None),
        P(DP, SP, None),
        P(SP, DP, None),
        P(SP, None),
        P(),
    )
    out_specs = (P(DP, SP, None), P(DP, SP, None), P(SP, DP, None), P(SP, DP), P())
    return jax.shard_map(
        shards, mesh=torus, in_specs=in_specs, out_specs=out_specs, check_vma=False
    )
```

```python
import functools
import math

import jax
import jax.numpy as jnp
from jax import lax
from jax.experimental import pallas as pl
from jax.experimental.pallas import tpu as pltpu
from jax.sharding import Mesh
from jax.sharding import PartitionSpec as P

Z = "sp_0"
SP = ("sp_0", "sp_1")
DP = ("dp_0", "dp_1")
PLANE = ("dp_0", "dp_1", "sp_1")
Z_DP = ("sp_0", "dp_0", "dp_1")

norm_floor = 0.5
root_half = 1.0 / math.sqrt(2.0)
inv_root_tau = 1.0 / math.sqrt(2.0 * math.pi)
LANES = 128
F32 = jnp.float32
BF16 = jnp.bfloat16


def normal_cdf(x):
    return 0.5 * (1.0 + lax.erf(x * root_half))


HBM = pl.BlockSpec(memory_space=pltpu.HBM)
VMEM = pl.BlockSpec(memory_space=pltpu.VMEM)


def limit(mib):
    return pltpu.CompilerParams(vmem_limit_bytes=mib * 1024 * 1024)


def params(mib):
    return pltpu.CompilerParams(
        dimension_semantics=("arbitrary",), vmem_limit_bytes=mib * 1024 * 1024
    )


def prologue_kernel(
    groups, rows, cot_hbm, up_hbm, val_hbm, gain_ref, out_hbm, inv_ref, cot_ref, up_ref, val_ref, out_ref, act_ref, sems
):
    toks = cot_ref.shape[0]
    steps = toks // rows

    def loads(i):
        at = pl.ds(pl.multiple_of(i * rows, rows), rows)
        pairs = ((cot_hbm, cot_ref), (up_hbm, up_ref), (val_hbm, val_ref))
        return [
            pltpu.make_async_copy(src.at[at], dst.at[at], sems.at[k, i])
            for k, (src, dst) in enumerate(pairs)
        ]

    def store(i):
        at = pl.ds(pl.multiple_of(i * rows, rows), rows)
        return pltpu.make_async_copy(out_ref.at[:, :, at], out_hbm.at[:, :, at], sems.at[3, i])

    for i in range(AHEAD):
        for copy in loads(i):
            copy.start()

    def step(i, carry):
        for copy in loads(i):
            copy.wait()

        @pl.when(i + AHEAD < steps)
        def _():
            for copy in loads(i + AHEAD):
                copy.start()

        at = pl.ds(pl.multiple_of(i * rows, rows), rows)

        def first(g, squares):
            cols = pl.ds(pl.multiple_of(g * LANES, LANES), LANES)
            up = up_ref[at, cols].astype(F32)
            up_act = (up * normal_cdf(up)).astype(BF16).astype(F32)
            out_ref[block_of(g), 0, at] = (cot_ref[at, cols].astype(F32) * up_act).astype(BF16)
            val = val_ref[at, cols].astype(F32)
            act = val * normal_cdf(val)
            act_ref[:, cols] = act
            return squares + act * act

        squares = lax.fori_loop(0, groups, first, jnp.zeros((rows, LANES), F32), unroll=UNROLL)
        mean = jnp.sum(squares, axis=1, keepdims=True) * (1.0 / (groups * LANES))
        inv = lax.rsqrt(mean + norm_floor)
        inv_ref[at] = jnp.broadcast_to(inv, (rows, LANES))

        def second(g, carry):
            cols = pl.ds(pl.multiple_of(g * LANES, LANES), LANES)
            out_ref[block_of(g), 1, at] = (act_ref[:, cols] * inv * gain_ref[:, cols]).astype(BF16)
            return carry

        lax.fori_loop(0, groups, second, 0, unroll=4)
        store(i).start()
        return carry

    lax.fori_loop(0, steps, step, 0)
    for i in range(steps):
        store(i).wait()


UNROLL = 4
AHEAD = 4


def prologue(cot, up, val, gain, rows=64):
    toks, width = cot.shape
    groups = width // LANES
    whole = pltpu.VMEM((toks, width), BF16)
    return pl.pallas_call(
        functools.partial(prologue_kernel, groups, rows),
        in_specs=[HBM, HBM, HBM, VMEM],
        out_specs=[HBM, VMEM],
        out_shape=[
            jax.ShapeDtypeStruct((groups, 2, toks, LANES), BF16),
            jax.ShapeDtypeStruct((toks, LANES), F32),
        ],
        scratch_shapes=[
            whole,
            whole,
            whole,
            pltpu.VMEM((groups, 2, toks, LANES), BF16),
            pltpu.VMEM((rows, width), F32),
            pltpu.SemaphoreType.DMA((4, toks // rows)),
        ],
        compiler_params=limit(60),
        cost_estimate=pl.CostEstimate(
            flops=100 * toks * width, bytes_accessed=10 * toks * width, transcendentals=0
        ),
        name="prologue",
    )(cot, up, val, gain)


def slopes_kernel(up_ref, val_ref, up_slope_ref, val_slope_ref, act_ref):
    groups = up_ref.shape[1] // LANES

    def step(g, carry):
        at = pl.ds(pl.multiple_of(g * LANES, LANES), LANES)
        up = up_ref[:, at].astype(F32)
        up_slope = normal_cdf(up) + up * (jnp.exp(-0.5 * up * up) * inv_root_tau)
        up_slope_ref[:, at] = up_slope.astype(BF16)
        val = val_ref[:, at].astype(F32)
        phi = normal_cdf(val)
        act_ref[:, at] = (val * phi).astype(BF16)
        val_slope = phi + val * (jnp.exp(-0.5 * val * val) * inv_root_tau)
        val_slope_ref[:, at] = val_slope.astype(BF16)
        return carry

    lax.fori_loop(0, groups, step, 0, unroll=2)


def slopes(up, val, rows=64):
    toks, width = up.shape
    row = pl.BlockSpec((rows, width), lambda i: (i, 0))
    out = jax.ShapeDtypeStruct((toks, width), BF16)
    return pl.pallas_call(
        slopes_kernel,
        grid=(toks // rows,),
        in_specs=[row, row],
        out_specs=[row, row, row],
        out_shape=[out, out, out],
        compiler_params=params(60),
        cost_estimate=pl.CostEstimate(
            flops=100 * toks * width, bytes_accessed=16 * toks * width, transcendentals=0
        ),
        name="slopes",
    )(up, val)


def column():
    return lax.axis_index("dp_1") * 4 + lax.axis_index("dp_0")


def place(column):
    return column % 4 * 2 + column // 4


def block_of(group):
    at = group >> 2
    return ((at & 3) * 2 + (at >> 2)) * 4 + (group & 3)


def slab_of(z_offset):
    return ((lax.axis_index(Z) + z_offset + 8) % 8) ^ column()


OFFSETS = (0, -1, -2, -3, 1, 2, 3, 4)
PAD = 8


def arrange_kernel(*refs):
    *pieces, w_ref, wt_ref = refs
    slab = pieces[0].shape[0]
    for d, piece in enumerate(pieces):
        at = pl.ds(pl.multiple_of(slab_of(OFFSETS[d]) * slab, slab), slab)
        rows = piece[...]
        w_ref[at] = rows
        wt_ref[:, at] = jnp.transpose(rows)


def arrange(pieces):
    _, block = pieces[0].shape
    return pl.pallas_call(
        arrange_kernel,
        in_specs=[VMEM] * len(pieces),
        out_specs=[VMEM] * 2,
        out_shape=[
            jax.ShapeDtypeStruct((block, block), BF16),
            jax.ShapeDtypeStruct((block, block), BF16),
        ],
        compiler_params=limit(8),
        cost_estimate=pl.CostEstimate(
            flops=4 * block * block, bytes_accessed=6 * block * block, transcendentals=0
        ),
        name="arrange",
    )(*pieces)


def mix_kernel(
    seqs, parts, per, recv_hbm, w_hbm, wt_hbm, bias_row_ref, out_hbm, sums_ref,
    recv_ref, out_ref, w_ref, wt_ref, bias_ref, sems, fixed_sems
):
    toks = recv_ref.shape[2]
    block = parts * toks
    steps = seqs // per

    def load(j):
        at = pl.ds(j * (per * parts), per * parts)
        return pltpu.make_async_copy(recv_hbm.at[at], recv_ref.at[at], sems.at[0, j])

    def store(j):
        at = pl.ds(j * per, per)
        return pltpu.make_async_copy(out_ref.at[at], out_hbm.at[at], sems.at[1, j])

    def side_by_side(j, which):
        return jnp.concatenate(
            [
                recv_ref[pl.ds((j * per + b) * parts, parts), which].reshape(block, LANES)
                for b in range(per)
            ],
            axis=1,
        )

    fixed = [
        pltpu.make_async_copy(src, dst, fixed_sems.at[k])
        for k, (src, dst) in enumerate(((wt_hbm, wt_ref), (w_hbm, w_ref)))
    ]
    fixed[0].start()
    load(0).start()
    fixed[1].start()
    for j in range(1, steps):
        load(j).start()
    bias_ref[...] = jnp.transpose(jnp.broadcast_to(bias_row_ref[...], (LANES, block)))
    fixed[0].wait()

    def step(j, total):
        load(j).wait()
        gate = side_by_side(j, 0)
        back = jnp.dot(wt_ref[...], gate, preferred_element_type=F32).astype(BF16)
        value = side_by_side(j, 1)
        for b in range(per):
            cols = slice(b * LANES, (b + 1) * LANES)
            out_ref[j * per + b, :, 1] = back[:, cols].reshape(parts, toks, LANES)
            terms = back[:, cols].astype(F32) * value[:, cols].astype(F32)
            total += jnp.sum(terms.reshape(block // 8, 8, LANES), axis=0)

        @pl.when(j == 0)
        def _():
            fixed[1].wait()

        mixed = jnp.dot(w_ref[...], value, preferred_element_type=F32)
        for b in range(per):
            cols = slice(b * LANES, (b + 1) * LANES)
            part = (mixed[:, cols] + bias_ref[...]).astype(BF16)
            out_ref[j * per + b, :, 0] = part.reshape(parts, toks, LANES)
        store(j).start()
        return total

    total = lax.fori_loop(0, steps, step, jnp.zeros((8, LANES), F32))
    sums_ref[...] = jnp.sum(total, axis=0, keepdims=True)
    for j in range(steps):
        store(j).wait()


PER = 4


def mix(recv, w, wt, bias, seqs, parts):
    toks = recv.shape[2]
    block = parts * toks
    whole = (seqs, parts, 2, toks, LANES)
    out, sums = pl.pallas_call(
        functools.partial(mix_kernel, seqs, parts, PER),
        in_specs=[HBM] * 3 + [VMEM],
        out_specs=[HBM, VMEM],
        out_shape=[jax.ShapeDtypeStruct(whole, BF16), jax.ShapeDtypeStruct((1, LANES), F32)],
        scratch_shapes=[
            pltpu.VMEM(recv.shape, BF16),
            pltpu.VMEM(whole, BF16),
            pltpu.VMEM((block, block), BF16),
            pltpu.VMEM((block, block), BF16),
            pltpu.VMEM((block, LANES), F32),
            pltpu.SemaphoreType.DMA((2, seqs // PER)),
            pltpu.SemaphoreType.DMA((2,)),
        ],
        compiler_params=limit(60),
        cost_estimate=pl.CostEstimate(
            flops=4 * block * block * seqs * LANES, bytes_accessed=10 * block * block, transcendentals=0
        ),
        name="mix",
    )(recv, w, wt, bias)
    return out.reshape(recv.shape), sums


def split(x):
    high = x.astype(BF16)
    middle = (x - high.astype(F32)).astype(BF16)
    low = (x - high.astype(F32) - middle.astype(F32)).astype(BF16)
    return high, middle, low


def pack_sums(sums):
    bias = split(sums[:, LANES:])
    wide = jnp.concatenate([sums[:, :LANES], jnp.zeros_like(sums[:, 2 * LANES :])], axis=1)
    gain = split(wide)
    zeros = jnp.zeros_like(bias[0])
    return jnp.concatenate([*bias, *gain, zeros, zeros], axis=0)


def unpack_sums(rows):
    rows = rows.astype(F32)
    bias = rows[0:1] + rows[1:2] + rows[2:3]
    gain = rows[3:4] + rows[4:5] + rows[5:6]
    return jnp.concatenate([gain[:, :LANES], bias], axis=1)


def grads_kernel(seqs, parts, recv_ref, sums_ref, *refs):
    outs = refs[:seqs]
    gate_ref, value_ref, grad_ref, rows_ref, sems = refs[seqs:]
    toks = recv_ref.shape[2]
    block = parts * toks
    slab = block // seqs
    for b in range(seqs):
        cols = slice(b * LANES, (b + 1) * LANES)
        pieces = slice(b * parts, (b + 1) * parts)
        pltpu.make_async_copy(recv_ref.at[pieces, 0], gate_ref.at[:, :, cols], sems.at[0, 0]).start()
        pltpu.make_async_copy(recv_ref.at[pieces, 1], value_ref.at[:, :, cols], sems.at[1, 0]).start()
    pltpu.make_async_copy(gate_ref, gate_ref, sems.at[0, 0]).wait()
    bias_sums = []
    for y in range(parts):
        gate = gate_ref[y].astype(F32)
        gate = sum(gate[:, b * LANES : (b + 1) * LANES] for b in range(seqs))
        bias_sums.append(jnp.sum(jnp.transpose(gate), axis=0, keepdims=True))
    rows_ref[...] = pack_sums(jnp.concatenate([sums_ref[...], *bias_sums], axis=1))
    for d in range(seqs):
        pltpu.make_async_copy(rows_ref, outs[d].at[slab:], sems.at[3, d]).start()
    pltpu.make_async_copy(value_ref, value_ref, sems.at[1, 0]).wait()

    def step(y, carry):
        grad = lax.dot_general(
            gate_ref[...].reshape(block, seqs * LANES),
            value_ref[y],
            (((1,), (1,)), ((), ())),
            preferred_element_type=F32,
        )
        grad_ref[y] = grad.astype(BF16)
        at = pl.ds(pl.multiple_of(y * toks, toks), toks)
        for d in range(seqs):
            rows = pl.ds(pl.multiple_of(slab_of(-OFFSETS[d]) * slab, slab), slab)
            pltpu.make_async_copy(grad_ref.at[y, rows], outs[d].at[:slab, at], sems.at[2, 0]).start()
        return carry

    lax.fori_loop(0, parts, step, 0)
    pltpu.make_async_copy(grad_ref, grad_ref, sems.at[2, 0]).wait()
    for d in range(seqs):
        pltpu.make_async_copy(rows_ref, outs[d].at[slab:], sems.at[3, d]).wait()


def weight_grads(recv, sums, seqs, parts):
    toks = recv.shape[2]
    block = parts * toks
    flat = pltpu.VMEM((parts, toks, seqs * LANES), BF16)
    return pl.pallas_call(
        functools.partial(grads_kernel, seqs, parts),
        in_specs=[HBM, VMEM],
        out_specs=[HBM] * seqs,
        out_shape=[jax.ShapeDtypeStruct((block // seqs + PAD, block), BF16)] * seqs,
        scratch_shapes=[
            flat,
            flat,
            pltpu.VMEM((parts, block, toks), BF16),
            pltpu.VMEM((PAD, block), BF16),
            pltpu.SemaphoreType.DMA((4, seqs)),
        ],
        compiler_params=limit(28),
        cost_estimate=pl.CostEstimate(
            flops=2 * block * block * seqs * LANES, bytes_accessed=6 * block * block, transcendentals=0
        ),
        name="weight_grads",
    )(recv, sums)


def hop_kernel(slab, *refs):
    n = len(refs) // 3
    for here, there, out in zip(refs[:n], refs[n : 2 * n], refs[2 * n :]):
        out[:slab] = (here[:slab].astype(F32) + there[:slab].astype(F32)).astype(BF16)
        out[slab:] = pack_sums(unpack_sums(here[slab:]) + unpack_sums(there[slab:]))


def hop(here, there):
    height, width = here[0].shape
    return pl.pallas_call(
        functools.partial(hop_kernel, height - PAD),
        in_specs=[VMEM] * (2 * len(here)),
        out_specs=[VMEM] * len(here),
        out_shape=[jax.ShapeDtypeStruct((height, width), BF16)] * len(here),
        compiler_params=limit(8),
        cost_estimate=pl.CostEstimate(
            flops=2 * height * width, bytes_accessed=12 * height * width, transcendentals=0
        ),
        name="hop",
    )(*here, *there)


def last_kernel(slab, *refs):
    *ins, grad_ref = refs
    grad_ref[...] = sum(r[:slab].astype(F32) for r in ins).astype(BF16)


def last(pieces):
    height, width = pieces[0].shape
    return pl.pallas_call(
        functools.partial(last_kernel, height - PAD),
        in_specs=[VMEM] * 3,
        out_specs=VMEM,
        out_shape=jax.ShapeDtypeStruct((height - PAD, width), BF16),
        compiler_params=limit(8),
        cost_estimate=pl.CostEstimate(
            flops=4 * height * width, bytes_accessed=8 * height * width, transcendentals=0
        ),
        name="last",
    )(*pieces)


def pack_kernel(slab, seqs, parts, *refs):
    *ins, gain_ref, small_ref = refs
    sums = sum(unpack_sums(r[slab:]) for r in ins)
    group = column() * parts + lax.axis_index("sp_1")
    gain = gain_ref[:, pl.ds(pl.multiple_of(group * LANES, LANES), LANES)]
    gain_sum = sums[:, :LANES] / gain
    small_ref[...] = jnp.zeros_like(small_ref)
    for a in range(seqs):
        at = slice((a + 1) * LANES, (a + 2) * LANES)
        for y in range(parts):
            small_ref[a * parts + y, :1] = gain_sum
            small_ref[a * parts + y, 1:2] = sums[:, at]


def pack(pieces, gain, seqs, parts):
    slab = pieces[0].shape[0] - PAD
    return pl.pallas_call(
        functools.partial(pack_kernel, slab, seqs, parts),
        in_specs=[VMEM] * 4,
        out_specs=VMEM,
        out_shape=jax.ShapeDtypeStruct((seqs * parts, 8, LANES), F32),
        compiler_params=limit(8),
        name="pack",
    )(*pieces, gain)


def unpack_kernel(parts, small_ref, gain_ref, bias_ref):
    for group in range(small_ref.shape[0]):
        gain_ref[group : group + 1] = small_ref[block_of(group), :1]
    mine = place(lax.axis_index(Z)) * parts + lax.axis_index("sp_1")
    bias_ref[...] = small_ref[mine, 1:2]


def unpack(small, parts):
    count = small.shape[0]
    gain, bias = pl.pallas_call(
        functools.partial(unpack_kernel, parts),
        in_specs=[VMEM],
        out_specs=[VMEM] * 2,
        out_shape=[
            jax.ShapeDtypeStruct((count, LANES), F32),
            jax.ShapeDtypeStruct((1, LANES), F32),
        ],
        compiler_params=limit(8),
        name="unpack",
    )(small)
    return gain.reshape(-1), bias


def epilogue_kernel(
    groups, rows, recv_hbm, cot_hbm, up_slope_hbm, val_slope_hbm, act_hbm, inv_ref, gain_ref, up_hbm, val_hbm,
    recv_ref, cot_ref, up_slope_ref, val_slope_ref, act_ref, up_ref, val_ref, sems
):
    toks = cot_ref.shape[0]
    steps = toks // rows

    def loads(i):
        at = pl.ds(pl.multiple_of(i * rows, rows), rows)
        pairs = (
            (cot_hbm, cot_ref),
            (up_slope_hbm, up_slope_ref),
            (val_slope_hbm, val_slope_ref),
            (act_hbm, act_ref),
        )
        return [pltpu.make_async_copy(recv_hbm.at[:, :, at], recv_ref.at[:, :, at], sems.at[0, i])] + [
            pltpu.make_async_copy(src.at[at], dst.at[at], sems.at[3 + k, i])
            for k, (src, dst) in enumerate(pairs)
        ]

    def stores(i):
        at = pl.ds(pl.multiple_of(i * rows, rows), rows)
        return [
            pltpu.make_async_copy(up_ref.at[at], up_hbm.at[at], sems.at[1, i]),
            pltpu.make_async_copy(val_ref.at[at], val_hbm.at[at], sems.at[2, i]),
        ]

    for i in range(AHEAD):
        for copy in loads(i):
            copy.start()

    def step(i, carry):
        for copy in loads(i):
            copy.wait()

        @pl.when(i + AHEAD < steps)
        def _():
            for copy in loads(i + AHEAD):
                copy.start()

        at = pl.ds(pl.multiple_of(i * rows, rows), rows)

        def first(g, dots):
            cols = pl.ds(pl.multiple_of(g * LANES, LANES), LANES)
            mid = (cot_ref[at, cols].astype(F32) * recv_ref[block_of(g), 0, at].astype(F32)).astype(BF16)
            up_ref[at, cols] = (mid.astype(F32) * up_slope_ref[at, cols].astype(F32)).astype(BF16)
            scaled = recv_ref[block_of(g), 1, at].astype(F32) * gain_ref[:, cols]
            return dots + scaled * act_ref[at, cols].astype(F32)

        dots = lax.fori_loop(0, groups, first, jnp.zeros((rows, LANES), F32), unroll=4)
        mean = jnp.sum(dots, axis=1, keepdims=True) * (1.0 / (groups * LANES))
        inv = inv_ref[at]
        pull = inv * inv * inv * mean

        def second(g, carry):
            cols = pl.ds(pl.multiple_of(g * LANES, LANES), LANES)
            scaled = recv_ref[block_of(g), 1, at].astype(F32) * gain_ref[:, cols]
            slope = inv * scaled - pull * act_ref[at, cols].astype(F32)
            val_ref[at, cols] = (slope * val_slope_ref[at, cols].astype(F32)).astype(BF16)
            return carry

        lax.fori_loop(0, groups, second, 0, unroll=4)
        for copy in stores(i):
            copy.start()
        return carry

    lax.fori_loop(0, steps, step, 0)
    for i in range(steps):
        for copy in stores(i):
            copy.wait()


def epilogue(recv, cot, up_slope, val_slope, act, inv, gain, rows=64):
    toks, width = cot.shape
    groups = width // LANES
    out = jax.ShapeDtypeStruct((toks, width), BF16)
    whole = pltpu.VMEM((toks, width), BF16)
    return pl.pallas_call(
        functools.partial(epilogue_kernel, groups, rows),
        in_specs=[HBM] * 5 + [VMEM] * 2,
        out_specs=[HBM, HBM],
        out_shape=[out, out],
        scratch_shapes=[
            pltpu.VMEM(recv.shape, BF16),
            whole,
            whole,
            whole,
            whole,
            whole,
            whole,
            pltpu.SemaphoreType.DMA((7, toks // rows)),
        ],
        compiler_params=limit(EPI_MIB),
        cost_estimate=pl.CostEstimate(
            flops=20 * toks * width, bytes_accessed=22 * toks * width, transcendentals=0
        ),
        name="epilogue",
    )(recv, cot, up_slope, val_slope, act, inv, gain)


EPI_MIB = 60


def shards(cotangent, up_pre, value_pre, spatial_weight, spatial_bias, value_gain):
    planes = lax.axis_size(Z)
    seqs = lax.axis_size(DP)
    parts = lax.axis_size("sp_1")
    cot, up, val = cotangent[0], up_pre[0], value_pre[0]
    gain = value_gain[None]
    away = [(z * seqs + a, (z ^ a) * seqs + place(z)) for z in range(planes) for a in range(seqs)]
    home = [(there, here) for here, there in away]

    def exchange(x):
        return lax.all_to_all(x, PLANE, split_axis=0, concat_axis=0, tiled=True)

    def shifted(x, by):
        return lax.ppermute(x, Z, [(z, (z + by) % planes) for z in range(planes)])

    bias = lax.ppermute(spatial_bias, Z_DP, away)
    weights = lax.ppermute(spatial_weight[0], Z_DP, away)
    sent, inv = prologue(cot, up, val, gain)
    recv = exchange(sent)
    before, after = [weights], [weights]
    for _ in range(3):
        before.append(shifted(before[-1], 1))
        after.append(shifted(after[-1], -1))
    after.append(shifted(after[-1], -1))
    pieces = before + after[1:]
    w, wt = arrange(pieces)
    back, sums = mix(recv, w, wt, bias, seqs, parts)
    back = exchange(back)
    own, p1, p2, p3, m1, m2, m3, m4 = weight_grads(recv, sums, seqs, parts)
    plus, minus = shifted(p3, 1), shifted(m4, -1)
    plus, minus = hop((p2, m3), (plus, minus))
    plus, minus = shifted(plus, 1), shifted(minus, -1)
    plus, minus = hop((p1, m2), (plus, minus))
    plus, minus = shifted(plus, 1), shifted(minus, -1)
    (minus,) = hop((m1,), (minus,))
    minus = shifted(minus, -1)
    grads = last((own, plus, minus))
    later_up, later_val, grads = lax.optimization_barrier((up, val, grads))
    up_slope, val_slope, act = slopes(later_up, later_val)
    small = pack((own, plus, minus), gain, seqs, parts)
    grads, up_slope = lax.optimization_barrier((grads, up_slope))
    grads = lax.ppermute(grads, Z_DP, home)
    small = exchange(small)
    gain_grad, bias_grad = unpack(small, parts)
    up_grad, value_grad = epilogue(back, cot, up_slope, val_slope, act, inv, gain)
    return (up_grad[None], value_grad[None], grads[None].astype(F32), bias_grad, gain_grad)


def solution(mesh):
    torus = Mesh(mesh.devices.reshape(8, 4, 4, 2), ("sp_0", "sp_1", "dp_0", "dp_1"))
    in_specs = (
        P(DP, SP, None),
        P(DP, SP, None),
        P(DP, SP, None),
        P(SP, DP, None),
        P(SP, None),
        P(),
    )
    out_specs = (P(DP, SP, None), P(DP, SP, None), P(SP, DP, None), P(SP, DP), P())
    return jax.shard_map(
        shards, mesh=torus, in_specs=in_specs, out_specs=out_specs, check_vma=False
    )
```
